256 devices in a mesh: ep: 16 (over y, x), tp: 16 (over z, core).
Axes of the slice: x: 4, y: 4, z: 8, core: 2. Of those that a mesh axis runs over, the one named last changes fastest.
Arguments:
- tokens: bfloat16 [1024, 2048], P('ep'), may hold values from -7 to 7
- state: float32 [1024, 32, 64, 64], P('ep', 'tp'), may hold values from -6 to 6
- routes: int32 [1024, 2], P('ep'), may hold values from 0 to 15, all different within a row; in each aligned block of 64 rows (0 to 63, 64 to 127, ...) at most 12 rows name the same one
- route_logits: float32 [1024, 2], P('ep'), may hold values from -4 to 4
- mix_gain: float32 [2048], replicated, may hold values from 0.1 to 1.9
- w_recept: bfloat16 [2048, 2048], P(None, 'tp')
- w_key: bfloat16 [2048, 2048], P(None, 'tp'), may hold values from -0.125 to 0.125
- w_value: bfloat16 [2048, 2048], P(None, 'tp'), may hold values from -0.125 to 0.125
- w_decay: bfloat16 [2048, 2048], P(None, 'tp'), may hold values from -0.125 to 0.125
- w_rate: bfloat16 [2048, 2048], P(None, 'tp'), may hold values from -0.125 to 0.125
- decay_base: float32 [2048], P('tp'), may hold values from -3 to 1
- rate_base: float32 [2048], P('tp'), may hold values from -3 to 3
- key_gain: float32 [2048], P('tp'), may hold values from 0.1 to 1.9
- group_gain: float32 [2048], P('tp'), may hold values from 0.1 to 1.9
- w_output: bfloat16 [2048, 2048], P('tp'), may hold values from -0.125 to 0.125
- ffn_gain: float32 [2048], replicated, may hold values from 0.1 to 1.9
- w_gate: bfloat16 [16, 2048, 7168], P('ep', None, 'tp'), may hold values from -0.125 to 0.125
- w_up: bfloat16 [16, 2048, 7168], P('ep', None, 'tp'), may hold values from -0.125 to 0.125
- w_down: bfloat16 [16, 7168, 2048], P('ep', 'tp'), may hold values from -0.0625 to 0.0625
Outputs:
- output: bfloat16 [1024, 2048], P('ep', 'tp')
- new_state: float32 [1024, 32, 64, 64], P('ep', 'tp')
The draws below stay inside these ranges and needn't reach their ends.
Inputs may be any that keep to these rules, and one draw needn't show every extreme that they name: `routes`: for each expert, the 64 tokens of one device group's rows name it in at most 12 of their rows; the 2 experts of a row differ.
All inputs are finite; a program needn't handle non-finite values.
Results may differ from the reference program's by a relative error of at most 0.0091.
Values may be sent and summed in bfloat16 or wider, within the bound.
A program may use at most 64 MiB of HBM per device.

```python
import math
from functools import partial
import jax
import jax.numpy as jnp
import numpy as np
from jax import lax

D = 2048
HEADS = 32
HEAD = 64
FF = 7168
TOPK = 2
SEQ_DEV = 64
SEQS = 1024
EXPERTS = 16
CAP = 12
N_EP = 16


def draw_tokens(key, part):
    noise_key = jax.random.fold_in(key, 11)
    columns = jnp.exp(jnp.linspace(jnp.log(0.25), 0.0, D)).astype(jnp.float32)
    values = jnp.clip(jax.random.normal(noise_key, (SEQS, D), jnp.float32), -5.0, 5.0) * columns[None, :]
    return values.astype(jnp.bfloat16)


def draw_w_recept(key, part):
    entry_key = jax.random.fold_in(key, 21)
    scale_key = jax.random.fold_in(key, 22)
    head_scale = jnp.exp(jax.random.uniform(scale_key, (HEADS,), jnp.float32, jnp.log(0.001), jnp.log(0.01)))
    column_scale = jnp.repeat(head_scale, HEAD) * jnp.sqrt(64.0 / HEAD) / jnp.sqrt(1.0 * D)
    entries = jnp.clip(jax.random.normal(entry_key, (D, D), jnp.float32), -4.0, 4.0)
    values = entries * column_scale[None, :]
    return values.astype(jnp.bfloat16)


def steps_of(stream_key, extent, split, smallest, high):
    def one(position, blocks):
        heights = jax.random.uniform(jax.random.fold_in(jax.random.fold_in(stream_key, 6), position), (blocks,), jnp.float32, smallest / len(split), high / len(split))
        return jnp.repeat(jnp.exp(heights), extent[position] // blocks).reshape((-1,) + (1,) * (len(extent) - position - 1))

    gain = one(*split[0])
    for cut in split[1:]:
        gain = gain * one(*cut)
    return gain


def deal_out(own_key, own, number, rows, amount, top, bound, lean):
    ranking = jax.random.permutation(own_key, amount)
    crowded, usual = shares(amount, rows * top, bound, lean, True), shares(amount, rows * top, bound, lean, False)
    places = jnp.arange(amount)

    def named(sizes, rotation):
        used = int((sizes > 0).sum())
        fixed = max(1, used // 4)
        moved = fixed + (places - fixed + rotation * (used - fixed)) % max(1, amount - fixed)
        return jnp.zeros((amount,), jnp.int32).at[ranking[jnp.where(places < fixed, places, moved)]].set(jnp.asarray(sizes, jnp.int32))

    sizes = jnp.where(number % 4 == 0, named(crowded, number // 4), named(usual, number - number // 4 - 1))
    mixed = jax.random.permutation(jax.random.fold_in(own, 3), amount)
    source_of, taker = mixed[0:amount // 2 * 2:2], mixed[1:amount // 2 * 2:2]
    room = jnp.minimum(sizes[source_of] - 1, bound - sizes[taker]) // 2
    room = jnp.where((source_of == ranking[0]) | (taker == ranking[0]) | (sizes[taker] == 0), 0, jnp.maximum(room, 0))
    moved = jax.random.randint(jax.random.fold_in(own, 4), (amount // 2,), 0, 1 << 20) % (room + 1)
    sizes = sizes.at[source_of].add(-moved).at[taker].add(moved)
    labels = jnp.searchsorted(jnp.cumsum(sizes), jnp.arange(rows * top), side="right").astype(jnp.int32)
    table = labels.reshape(top, rows).T
    table = table[jax.random.permutation(jax.random.fold_in(own, 1), rows)]
    rotation = jax.random.randint(jax.random.fold_in(own, 2), (rows, 1), 0, top)
    return jnp.take_along_axis(table, (jnp.arange(top)[None, :] + rotation) % top, axis=1)


def shares(amount, total, bound, lean, full):
    portions = [(1 << 20) // math.isqrt(rank ** lean) + 1 for rank in range(1, amount + 1)]
    largest = bound if full else min(bound, max(-(-total // amount), total * portions[0] // sum(portions)))
    least = 1 if total - largest >= amount - 1 else 0
    given, rest = [largest] + [least] * (amount - 1), total - largest - least * (amount - 1)
    while rest > 0:
        movable = [i for i in range(1, amount) if given[i] < largest] or [i for i in range(1, amount) if given[i] < bound]
        pool, budget = sum([portions[i] for i in movable]), rest
        for i in movable:
            more = min(bound - given[i], max(1, budget * portions[i] // pool), rest)
            given[i] = given[i] + more
            rest = rest - more
    return np.array(given)


def noise(key, dims, width, limit, cuts=(), kind=jnp.bfloat16):
    drawn = width * jax.random.normal(key, dims, jnp.float32)
    if cuts:
        drawn = drawn * steps_of(key, dims, cuts, -0.22, 0.18)
    return jnp.clip(drawn, -limit, limit).astype(kind)


def setup_inputs(seed: int = 0) -> dict:
    key_of = jax.random.split(jax.random.key(seed), 20)
    tokens = draw_tokens(jax.random.fold_in(key_of[19], 71), 0)
    state = noise(key_of[1], (SEQS, HEADS, HEAD, HEAD), 1.0, 6.0, ((0, 16), (1, 16)), jnp.float32)
    routes_keys = jax.random.split(jax.random.fold_in(key_of[2], 1), SEQS // SEQ_DEV)
    routes_turns = jax.random.permutation(jax.random.fold_in(key_of[2], 3), SEQS // SEQ_DEV)
    routes = jax.vmap(lambda own, number: deal_out(jax.random.fold_in(key_of[2], 2), own, number, SEQ_DEV, EXPERTS, TOPK, CAP, 2))(routes_keys, routes_turns).reshape((SEQS, TOPK))
    route_logits = noise(key_of[3], (SEQS, TOPK), 1.5, 4.0, ((0, 16),), jnp.float32)
    mix_gain = jnp.clip(1.0 + 0.18 * jax.random.normal(key_of[4], (D,), jnp.float32), 0.1, 1.9)
    w_recept = draw_w_recept(jax.random.fold_in(key_of[19], 71), 0)
    w_key = noise(key_of[6], (D, D), D ** -0.5, 0.125, ((1, 16),))
    w_value = noise(key_of[7], (D, D), D ** -0.5, 0.125, ((1, 16),))
    w_decay = noise(key_of[8], (D, D), D ** -0.5, 0.125, ((1, 16),))
    w_rate = noise(key_of[9], (D, D), D ** -0.5, 0.125, ((1, 16),))
    decay_base = jnp.clip(-3.0 + 4.0 * jax.random.uniform(key_of[10], (D,), jnp.float32) ** steps_of(key_of[10], (D,), ((0, 16),), -0.2, 0.2), -3.0, 1.0)
    rate_base = noise(key_of[11], (D,), 1.0, 3.0, ((0, 16),), jnp.float32)
    key_gain = jnp.clip(1.0 + 0.18 * jax.random.normal(key_of[12], (D,), jnp.float32), 0.1, 1.9)
    group_gain = jnp.clip(1.0 + 0.18 * jax.random.normal(key_of[13], (D,), jnp.float32), 0.1, 1.9)
    w_output = noise(key_of[14], (D, D), D ** -0.5, 0.125, ((0, 16),))
    ffn_gain = jnp.clip(1.0 + 0.18 * jax.random.normal(key_of[15], (D,), jnp.float32), 0.1, 1.9)
    w_gate = noise(key_of[16], (EXPERTS, D, FF), D ** -0.5, 0.125, ((0, 16), (2, 16)))
    w_up = noise(key_of[17], (EXPERTS, D, FF), D ** -0.5, 0.125, ((0, 16), (2, 16)))
    w_down = noise(key_of[18], (EXPERTS, FF, D), FF ** -0.5, 0.0625, ((0, 16), (1, 16)))
    return {"tokens": tokens, "state": state, "routes": routes, "route_logits": route_logits, "mix_gain": mix_gain, "w_recept": w_recept, "w_key": w_key, "w_value": w_value, "w_decay": w_decay, "w_rate": w_rate, "decay_base": decay_base, "rate_base": rate_base, "key_gain": key_gain, "group_gain": group_gain, "w_output": w_output, "ffn_gain": ffn_gain, "w_gate": w_gate, "w_up": w_up, "w_down": w_down}


RMS_EPS = 1e-06
GROUP_EPS = 0.00064
UNIT_EPS = 6.4e-05
HIGHEST = lax.Precision.HIGHEST

def rounded(values):
    return lax.optimization_barrier(values.astype(jnp.bfloat16)).astype(jnp.float32)

def mix_heads(normed, state, w_recept, w_key, w_value, w_decay, w_rate, decay_base, rate_base, key_gain, group_gain):
    seq_rows = state.shape[0]
    head_count = state.shape[1]

    def project(weight):
        return rounded(jnp.dot(normed, weight, preferred_element_type=jnp.float32))

    def split_heads(values):
        return values.reshape(seq_rows, head_count, -1)
    recept = split_heads(project(w_recept))
    keys_now = split_heads(project(w_key))
    values_now = split_heads(project(w_value))
    decay_pre = project(w_decay) + decay_base
    decay_now = split_heads(jnp.exp(-jnp.exp(-jax.nn.softplus(-decay_pre) - 0.5)))
    rate_now = split_heads(jax.nn.sigmoid(project(w_rate) + rate_base))
    scaled = keys_now * key_gain.reshape(head_count, -1)[None]
    unit_key = scaled * lax.rsqrt(lax.optimization_barrier(jnp.sum(scaled * scaled, axis=2, keepdims=True)) + UNIT_EPS)
    removed = jnp.einsum('bhvk,bhk->bhv', state, unit_key, precision=HIGHEST)
    new_state = state * decay_now[:, :, None, :] - removed[:, :, :, None] * (unit_key * rate_now)[:, :, None, :] + values_now[:, :, :, None] * keys_now[:, :, None, :]
    readout = jnp.einsum('bhvk,bhk->bhv', new_state, recept, precision=HIGHEST)
    centred = readout - lax.optimization_barrier(jnp.mean(readout, axis=2, keepdims=True))
    spread = lax.optimization_barrier(jnp.mean(centred * centred, axis=2, keepdims=True))
    normed_read = centred * lax.rsqrt(spread + GROUP_EPS) * group_gain.reshape(head_count, -1)[None]
    return (normed_read.reshape(seq_rows, -1).astype(jnp.bfloat16), new_state)

def slot_numbers(route_rows, expert_count, capacity):
    flat_routes = route_rows.reshape(-1)
    one_hot = (flat_routes[:, None] == jnp.arange(expert_count, dtype=jnp.int32)[None, :]).astype(jnp.int32)
    earlier = jnp.cumsum(one_hot, axis=0) - one_hot
    placed = lax.optimization_barrier(jnp.sum(earlier * one_hot, axis=1)).astype(jnp.int32)
    return (flat_routes * capacity + placed).reshape(route_rows.shape)

def expert_rows(slot_rows, gate_weight, up_weight, down_weight):
    gate_act = jnp.dot(slot_rows, gate_weight, preferred_element_type=jnp.float32)
    upward = jnp.dot(slot_rows, up_weight, preferred_element_type=jnp.float32)
    hidden = (jax.nn.silu(gate_act) * upward).astype(jnp.bfloat16)
    return jnp.dot(hidden, down_weight, preferred_element_type=jnp.float32)

def reference(tokens, state, routes, route_logits, mix_gain, w_recept, w_key, w_value, w_decay, w_rate, decay_base, rate_base, key_gain, group_gain, w_output, ffn_gain, w_gate, w_up, w_down):
    values = tokens.astype(jnp.float32)
    normed = (values * lax.rsqrt(lax.optimization_barrier(jnp.mean(values * values, axis=1, keepdims=True)) + RMS_EPS) * mix_gain).astype(jnp.bfloat16)
    mixed_rows, new_state = mix_heads(normed, state, w_recept, w_key, w_value, w_decay, w_rate, decay_base, rate_base, key_gain, group_gain)
    residual = (values + jnp.dot(mixed_rows, w_output, preferred_element_type=jnp.float32)).astype(jnp.bfloat16)
    resid_vals = residual.astype(jnp.float32)
    ffn_in = (resid_vals * lax.rsqrt(lax.optimization_barrier(jnp.mean(resid_vals * resid_vals, axis=1, keepdims=True)) + RMS_EPS) * ffn_gain).astype(jnp.bfloat16)
    route_exp = jnp.exp(route_logits)
    route_weight = route_exp / lax.optimization_barrier(jnp.sum(route_exp, axis=1, keepdims=True))
    group_routes = routes.reshape(N_EP, SEQ_DEV, TOPK)
    slot_ids = jax.vmap(partial(slot_numbers, expert_count=EXPERTS, capacity=CAP))(group_routes)
    group_index = jnp.arange(N_EP, dtype=jnp.int32)
    local_token = jnp.broadcast_to(jnp.arange(SEQ_DEV, dtype=jnp.int32)[None, :, None], slot_ids.shape)
    global_token = local_token + (group_index * SEQ_DEV)[:, None, None]
    slot_flat = (slot_ids + (group_index * (EXPERTS * CAP))[:, None, None]).reshape(-1)
    owners_table = jnp.full((N_EP * EXPERTS * CAP,), SEQS, jnp.int32).at[slot_flat].set(global_token.reshape(-1))
    owners_table = owners_table.reshape(N_EP, EXPERTS, CAP).transpose(1, 0, 2).reshape(EXPERTS, N_EP * CAP)
    padded_in = jnp.concatenate([ffn_in, jnp.zeros((1, D), ffn_in.dtype)], axis=0)

    def one_expert(inputs):
        owners, gate_weight, up_weight, down_weight = inputs
        return expert_rows(padded_in[owners], gate_weight, up_weight, down_weight)
    outputs = lax.map(one_expert, (owners_table, w_gate, w_up, w_down)).reshape(EXPERTS, N_EP, CAP, D)
    place_in = (slot_ids - group_routes * CAP).astype(jnp.int32)
    picked = outputs[group_routes, group_index[:, None, None], place_in]
    moe_sum = lax.optimization_barrier(jnp.sum(picked * route_weight.reshape(N_EP, SEQ_DEV, TOPK)[..., None], axis=2)).reshape(SEQS, D)
    output = (resid_vals + moe_sum).astype(jnp.bfloat16)
    return (output, new_state)
```

```python
import jax
import jax.numpy as jnp
from jax import lax
from jax.experimental import pallas as pl
from jax.experimental.pallas import tpu as pltpu
from jax.sharding import PartitionSpec as P

MESH = pl.DeviceIdType.MESH
RMS_EPS = 1e-06
GROUP_EPS = 0.00064
UNIT_EPS = 6.4e-05
F32 = jnp.float32
BF16 = jnp.bfloat16

LANES = 128
HALF = 64
SIDE = 4
CHUNKS = 8
MAIN = 8
REST = 4

NEAR = sorted(range(SIDE * SIDE), key=lambda o: sum(min(d, SIDE - d) for d in divmod(o, SIDE)))


def dot(a, b, contract=((1,), (0,))):
    return lax.dot_general(a, b, (contract, ((), ())), preferred_element_type=F32)


def mixer_kernel(
    tok_hbm,
    st_hbm,
    mix_gain,
    w_recept,
    w_key,
    w_value,
    w_decay,
    w_rate,
    decay_base,
    rate_base,
    key_gain,
    group_gain,
    mixed_ref,
    ns_hbm,
    tok_v,
    w_v,
    st_v,
    ns_v,
    rows_v,
    read_v,
    tok_sem,
    w_sem,
    st_sem,
    ns_sem,
):
    seqs = tok_v.shape[0]
    per = seqs // CHUNKS
    tok_copy = pltpu.make_async_copy(tok_hbm, tok_v, tok_sem)
    tok_copy.start()
    w_copies = []
    for j, w_hbm in enumerate((w_recept, w_key, w_value, w_decay, w_rate)):
        copy = pltpu.make_async_copy(w_hbm, w_v.at[:, pl.ds(j * LANES, LANES)], w_sem.at[j])
        copy.start()
        w_copies.append(copy)

    def st_copy(i):
        part = pl.ds(i * per, per)
        return pltpu.make_async_copy(st_hbm.at[part], st_v.at[part], st_sem.at[i])

    def ns_copy(i):
        part = pl.ds(i * per, per)
        return pltpu.make_async_copy(ns_v.at[part], ns_hbm.at[part], ns_sem.at[i])

    for i in range(CHUNKS):
        st_copy(i).start()

    lane = lax.broadcasted_iota(jnp.int32, (seqs, LANES), 1)

    def per_head(values):
        first = jnp.sum(jnp.where(lane < HALF, values, 0.0), axis=1, keepdims=True)
        second = jnp.sum(jnp.where(lane < HALF, 0.0, values), axis=1, keepdims=True)
        return jnp.where(lane < HALF, first, second)

    tok_copy.wait()
    values = tok_v[...].astype(F32)
    scale = lax.rsqrt(jnp.mean(values * values, axis=1, keepdims=True) + RMS_EPS)
    normed = (values * scale * mix_gain[...]).astype(BF16)
    for copy in w_copies:
        copy.wait()
    projected = dot(normed, w_v[...]).astype(BF16).astype(F32)
    recept, key, value, decay_in, rate_in = (
        projected[:, j * LANES : (j + 1) * LANES] for j in range(5)
    )
    decay = jnp.exp(-(0.6065306597126334 * jax.nn.sigmoid(decay_in + decay_base[...])))
    rate = jax.nn.sigmoid(rate_in + rate_base[...])
    scaled = key * key_gain[...]
    unit = scaled * lax.rsqrt(per_head(scaled * scaled) + UNIT_EPS)
    rows_v[0] = unit
    rows_v[1] = decay
    rows_v[2] = unit * rate
    rows_v[3] = key
    rows_v[4] = recept
    rows_v[5] = value

    wide = 2 * LANES
    block_r = lax.broadcasted_iota(jnp.int32, (wide, wide), 0) // HALF
    block_c = lax.broadcasted_iota(jnp.int32, (wide, wide), 1) // HALF
    ones2 = (block_r == block_c).astype(BF16)
    ones1 = ones2[:LANES, :LANES]
    diag = (
        lax.broadcasted_iota(jnp.int32, (HALF, LANES), 0)
        == lax.broadcasted_iota(jnp.int32, (HALF, LANES), 1) % HALF
    )[None]

    def chunk(i, carry):
        st_copy(i).wait()
        part = pl.ds(pl.multiple_of(i * per, per), per)
        old = jnp.concatenate([st_v[part, 0], st_v[part, 1]], axis=-1)
        unit_c, decay_c, take_c, key_c, recept_c, value_c = (
            rows_v[j, part][:, None, :] for j in range(6)
        )
        probe = (old * unit_c).astype(BF16).reshape(per * HALF, LANES)
        spread = jnp.where(diag, value_c, 0.0).astype(BF16).reshape(per * HALF, LANES)
        both = dot(jnp.concatenate([probe, spread], axis=1), ones2)
        removed = both[:, :LANES].reshape(per, HALF, LANES)
        value_b = both[:, LANES:].reshape(per, HALF, LANES)
        new = old * decay_c - removed * take_c + value_b * key_c
        ns_v[part, 0] = new[..., :HALF]
        ns_v[part, 1] = new[..., HALF:]
        ns_copy(i).start()
        seen = dot((new * recept_c).astype(BF16).reshape(per * HALF, LANES), ones1)
        seen = jnp.where(diag, seen.reshape(per, HALF, LANES), 0.0)
        read_v[part, :] = jnp.sum(seen, axis=1)
        return carry

    lax.fori_loop(0, CHUNKS, chunk, 0)
    readout = read_v[...]
    centred = readout - per_head(readout) * (1.0 / HALF)
    spread = per_head(centred * centred) * (1.0 / HALF)
    mixed_ref[...] = (centred * lax.rsqrt(spread + GROUP_EPS) * group_gain[...]).astype(BF16)
    for i in range(CHUNKS):
        ns_copy(i).wait()


def expert_kernel(
    mixed_ref,
    tok_ref,
    routes_ref,
    logits_ref,
    gain_ref,
    wo_hbm,
    wg_hbm,
    wu_hbm,
    wd_hbm,
    out_ref,
    wo_v,
    wg_v,
    wu_v,
    wd_v,
    pair_send,
    pair_recv,
    own_v,
    rs_send,
    rs_recv,
    resid_v,
    disp_send,
    x_recv,
    xs_v,
    y_send,
    y_recv,
    yown_v,
    ret_send,
    ret_recv,
    moe_send,
    moe_recv,
    w_sem,
    wo_sem,
    wd_sem,
    pair_sem,
    rs_ssem,
    rs_rsem,
    ag_ssem,
    ag_rsem,
    disp_ssem,
    disp_rsem,
    relay_ssem,
    relay_rsem,
    y_sem,
    ret_ssem,
    ret_rsem,
    moe_ssem,
    moe_rsem,
):
    depth = lax.axis_size("tp") // 2
    rows = tok_ref.shape[0]
    groups = SIDE * SIDE
    ep = lax.axis_index("ep")
    tp = lax.axis_index("tp")
    z, core = tp // 2, tp % 2
    y, x = ep // SIDE, ep % SIDE
    other = 1 - core

    def along(dz):
        return (ep, ((z + dz) % depth) * 2 + core)

    def plane(o, sign):
        dy, dx = divmod(o, SIDE)
        to_y = (y + sign * dy + SIDE) % SIDE
        to_x = (x + sign * dx + SIDE) % SIDE
        return (to_y * SIDE + to_x, tp)

    partner = (ep, z * 2 + other)

    def send(src, dst, ssem, rsem, target):
        return pltpu.make_async_remote_copy(
            src_ref=src,
            dst_ref=dst,
            send_sem=ssem,
            recv_sem=rsem,
            device_id=target,
            device_id_type=MESH,
        )

    barrier = pltpu.get_barrier_semaphore()
    peers = [partner] + [along(dz) for dz in range(1, depth)]
    peers += [plane(o, 1) for o in range(1, groups)]
    for peer in peers:
        pl.semaphore_signal(barrier, inc=1, device_id=peer, device_id_type=MESH)

    wo_copies, wd_copies = [], []
    for j in range(2 * depth):
        cols = pl.ds(j * LANES, LANES)
        half = pl.ds((j // 2) * LANES, LANES)
        copy = pltpu.make_async_copy(wo_hbm.at[:, cols], wo_v.at[j % 2, :, half], wo_sem.at[j])
        copy.start()
        wo_copies.append(copy)
    gate_copy = pltpu.make_async_copy(wg_hbm, wg_v, w_sem.at[0])
    up_copy = pltpu.make_async_copy(wu_hbm, wu_v, w_sem.at[1])
    gate_copy.start()
    up_copy.start()
    for j in range(2 * depth):
        cols = pl.ds(j * LANES, LANES)
        half = pl.ds((j // 2) * LANES, LANES)
        copy = pltpu.make_async_copy(wd_hbm.at[:, cols], wd_v.at[j % 2, :, half], wd_sem.at[j])
        copy.start()
        wd_copies.append(copy)

    for copy in wo_copies:
        copy.wait()
    mixed = mixed_ref[...]
    theirs = dot(mixed, wo_v[other]).astype(BF16)
    for k in range(depth):
        pair_send[k] = theirs[:, k * LANES : (k + 1) * LANES]
    pl.semaphore_wait(barrier, len(peers))
    pair_copy = send(pair_send, pair_recv, pair_sem.at[0], pair_sem.at[1], partner)
    pair_copy.start()
    mine = dot(mixed, wo_v[core])
    for k in range(depth):
        own_v[k] = mine[:, k * LANES : (k + 1) * LANES]
    pair_copy.wait_recv()

    far = sorted(range(1, depth), key=lambda dz: -min(dz, depth - dz))
    rs_copies = {}
    for dz in far:
        k = (z + dz) % depth
        rs_send[dz] = (own_v[k] + pair_recv[k].astype(F32)).astype(BF16)
        copy = send(rs_send.at[dz], rs_recv.at[dz], rs_ssem.at[dz], rs_rsem.at[dz], along(dz))
        copy.start()
        rs_copies[dz] = copy
    cols = pl.ds(pl.multiple_of(tp * LANES, LANES), LANES)
    total = own_v[z] + pair_recv[z].astype(F32)

    row16 = lax.broadcasted_iota(jnp.int32, (groups, rows), 0)
    expert = (((y + (row16 >> 2)) & 3) << 2) | ((x + (row16 & 3)) & 3)
    first = (routes_ref[0:1, :] == expert).astype(BF16)
    second = (routes_ref[1:2, :] == expert).astype(BF16)
    before = (
        lax.broadcasted_iota(jnp.int32, (rows, rows), 0)
        < lax.broadcasted_iota(jnp.int32, (rows, rows), 1)
    ).astype(BF16)
    rank = dot(first + second, before).astype(BF16)
    slots = groups * MAIN
    expand = (
        (lax.broadcasted_iota(jnp.int32, (slots, groups), 0) // MAIN)
        == lax.broadcasted_iota(jnp.int32, (slots, groups), 1)
    ).astype(BF16)
    first_x = dot(expand, first)
    second_x = dot(expand, second)
    rank_x = dot(expand, rank).astype(jnp.int32)
    slot = lax.broadcasted_iota(jnp.int32, (slots, rows), 0) % MAIN
    named = (first_x + second_x) > 0.5
    pick_main = jnp.where(named & (rank_x == slot), 1.0, 0.0)
    pick_low = jnp.where(named & (rank_x == slot + MAIN) & (slot < REST), 1.0, 0.0)
    pick_high = jnp.where(named & (rank_x == slot + REST) & (slot >= REST), 1.0, 0.0)
    exp0 = jnp.exp(logits_ref[0:1, :])
    exp1 = jnp.exp(logits_ref[1:2, :])
    weight = (first_x * exp0 + second_x * exp1) / (exp0 + exp1)

    def split(table):
        turned = (table * weight).T
        top = turned.astype(BF16)
        return top, (turned - top.astype(F32)).astype(BF16)

    give_main, give_low, give_high = split(pick_main), split(pick_low), split(pick_high)
    pick_main, pick_low, pick_high = (t.astype(BF16) for t in (pick_main, pick_low, pick_high))

    for dz in reversed(far):
        rs_copies[dz].wait_recv()
        total = total + rs_recv[dz].astype(F32)
    own_resid = (tok_ref[:, cols].astype(F32) + total).astype(BF16)
    resid_v[z] = own_resid
    ag_copies = []
    for dz in far:
        copy = send(resid_v.at[z], resid_v.at[z], ag_ssem.at[dz], ag_rsem.at[dz], along(dz))
        copy.start()
        ag_copies.append(copy)
    for dz in reversed(far):
        src = resid_v.at[(z - dz + depth) % depth]
        send(src, src, ag_ssem.at[dz], ag_rsem.at[dz], along(dz)).wait_recv()

    half_cols = depth * LANES
    quarter = half_cols // 2
    resid = jnp.concatenate([resid_v[k] for k in range(depth)], axis=1)
    picked = dot(pick_main, resid).astype(BF16).reshape(groups, MAIN, half_cols)
    low = dot(pick_low, resid[:, :quarter]) + dot(pick_high, resid[:, quarter:])
    low = low.astype(BF16).reshape(groups, MAIN, quarter)
    disp_send[:, :, 0:half_cols] = picked
    disp_send[:, :, half_cols:] = low
    x_recv[core, 0] = disp_send[0]
    disp_copies = {}
    for o in reversed(NEAR[1:]):
        copy = send(
            disp_send.at[o], x_recv.at[core, o], disp_ssem.at[o], disp_rsem.at[o], plane(o, 1)
        )
        copy.start()
        disp_copies[o] = copy
    relays = []
    for o in NEAR:
        src = disp_send.at[0]
        if o:
            disp_copies[o].wait_recv()
            src = x_recv.at[core, o]
        copy = send(src, x_recv.at[core, o], relay_ssem.at[o], relay_rsem.at[o], partner)
        copy.start()
        relays.append(copy)
    for o in NEAR:
        dst = x_recv.at[other, o]
        send(dst, dst, relay_ssem.at[o], relay_rsem.at[o], partner).wait_recv()

    main_rows = groups * MAIN
    all_rows = main_rows + groups * REST
    tile_row = lax.broadcasted_iota(jnp.int32, (groups // 2, MAIN, quarter), 1)
    upper = tile_row < REST
    halves_main, halves_rest = [], []
    for p in range(2):
        block = x_recv[p].astype(F32)
        halves_main.append(block[:, :, :half_cols].reshape(main_rows, half_cols))
        rest = block[:, :, half_cols:].reshape(groups // 2, 2, MAIN, quarter)
        a, b = rest[:, 0], rest[:, 1]
        lower_cols = jnp.where(upper, a, pltpu.roll(b, REST, 1))
        upper_cols = jnp.where(upper, pltpu.roll(a, REST, 1), b)
        joined = jnp.concatenate([lower_cols, upper_cols], axis=2)
        halves_rest.append(joined.reshape(all_rows - main_rows, half_cols))
    width = 2 * half_cols
    for start, halves in ((0, halves_main), (main_rows, halves_rest)):
        count = halves[0].shape[0]
        squares = sum(jnp.sum(h * h, axis=1, keepdims=True) for h in halves)
        scale = lax.rsqrt(squares * (1.0 / width) + RMS_EPS)
        for p in range(2):
            for k in range(depth):
                at = (2 * k + p) * LANES
                piece = halves[p][:, k * LANES : (k + 1) * LANES] * scale
                piece = piece * gain_ref[:, at : at + LANES]
                xs_v[start : start + count, at : at + LANES] = piece.astype(BF16)

    gate_copy.wait()
    up_copy.wait()
    for copy in wd_copies:
        copy.wait()
    xs = xs_v[...]
    gate = dot(xs, wg_v[...], ((1,), (1,)))
    up = dot(xs, wu_v[...], ((1,), (1,)))
    hidden = (gate * jax.nn.sigmoid(gate) * up).astype(BF16)
    y_send[...] = dot(hidden, wd_v[other]).astype(BF16)
    y_copy = send(y_send, y_recv, y_sem.at[0], y_sem.at[1], partner)
    y_copy.start()
    yown_v[...] = dot(hidden, wd_v[core])
    y_copy.wait_recv()

    summed = yown_v[...] + y_recv[...].astype(F32)
    ret_send[:, :, 0:half_cols] = (
        summed[:main_rows].astype(BF16).reshape(groups, MAIN, half_cols)
    )
    rest = summed[main_rows:].reshape(groups // 2, MAIN, half_cols)
    lower_cols, upper_cols = rest[:, :, :quarter], rest[:, :, quarter:]
    a = jnp.where(upper, lower_cols, pltpu.roll(upper_cols, REST, 1))
    b = jnp.where(upper, pltpu.roll(lower_cols, REST, 1), upper_cols)
    for p in range(groups // 2):
        ret_send[2 * p, :, half_cols:] = a[p].astype(BF16)
        ret_send[2 * p + 1, :, half_cols:] = b[p].astype(BF16)
    ret_recv[0] = ret_send[0]
    ret_copies = {}
    for o in reversed(NEAR[1:]):
        copy = send(ret_send.at[o], ret_recv.at[o], ret_ssem.at[o], ret_rsem.at[o], plane(o, -1))
        copy.start()
        ret_copies[o] = copy
    for o in NEAR[1:]:
        ret_copies[o].wait_recv()

    back = ret_recv[...]
    back_main = back[:, :, :half_cols].reshape(slots, half_cols)
    back_rest = back[:, :, half_cols:].reshape(slots, quarter)

    def give(tables, data):
        return dot(tables[0], data) + dot(tables[1], data)

    moe = give(give_main, back_main)
    moe_low = moe[:, :quarter] + give(give_low, back_rest)
    moe_high = moe[:, quarter:] + give(give_high, back_rest)
    moe = jnp.concatenate([moe_low, moe_high], axis=1)
    for k in range(depth):
        own_v[k] = moe[:, k * LANES : (k + 1) * LANES]
    moe_copies = {}
    for dz in far:
        moe_send[dz] = own_v[(z + dz) % depth].astype(BF16)
        copy = send(moe_send.at[dz], moe_recv.at[dz], moe_ssem.at[dz], moe_rsem.at[dz], along(dz))
        copy.start()
        moe_copies[dz] = copy
    total = own_resid.astype(F32) + own_v[z]
    for dz in reversed(far):
        moe_copies[dz].wait_recv()
        total = total + moe_recv[dz].astype(F32)
    out_ref[...] = total.astype(BF16)

    sent = [pair_copy, y_copy] + ag_copies + relays
    for group in (rs_copies, disp_copies, ret_copies, moe_copies):
        sent += list(group.values())
    for copy in sent:
        copy.wait_send()


def local(
    tokens,
    state,
    routes,
    route_logits,
    mix_gain,
    w_recept,
    w_key,
    w_value,
    w_decay,
    w_rate,
    decay_base,
    rate_base,
    key_gain,
    group_gain,
    w_output,
    ffn_gain,
    w_gate,
    w_up,
    w_down,
):
    seqs, width = tokens.shape
    hidden = w_gate.shape[2]
    vmem = pl.BlockSpec(memory_space=pltpu.VMEM)
    anywhere = pl.BlockSpec(memory_space=pl.ANY)
    dma = pltpu.SemaphoreType.DMA

    def row(vector):
        return vector.reshape(1, -1)

    mixed, new_state = pl.pallas_call(
        mixer_kernel,
        out_shape=(
            jax.ShapeDtypeStruct((seqs, LANES), BF16),
            jax.ShapeDtypeStruct(state.shape, F32),
        ),
        in_specs=[anywhere, anywhere, vmem] + [anywhere] * 5 + [vmem] * 4,
        out_specs=(vmem, anywhere),
        scratch_shapes=[
            pltpu.VMEM((seqs, width), BF16),
            pltpu.VMEM((width, 5 * LANES), BF16),
            pltpu.VMEM(state.shape, F32),
            pltpu.VMEM(state.shape, F32),
            pltpu.VMEM((6, seqs, LANES), F32),
            pltpu.VMEM((seqs, LANES), F32),
            dma(()),
            dma((5,)),
            dma((CHUNKS,)),
            dma((CHUNKS,)),
        ],
        compiler_params=pltpu.CompilerParams(vmem_limit_bytes=40 * 2**20),
        name="mixer",
    )(
        tokens,
        state,
        row(mix_gain),
        w_recept,
        w_key,
        w_value,
        w_decay,
        w_rate,
        row(decay_base),
        row(rate_base),
        row(key_gain),
        row(group_gain),
    )

    depth = lax.axis_size("tp") // 2
    groups = SIDE * SIDE
    half_cols = depth * LANES
    message = half_cols + half_cols // 2
    all_rows = groups * (MAIN + REST)
    block = (depth, seqs, LANES)
    output = pl.pallas_call(
        expert_kernel,
        out_shape=jax.ShapeDtypeStruct((seqs, LANES), BF16),
        in_specs=[vmem] * 5 + [anywhere] * 4,
        out_specs=vmem,
        scratch_shapes=[
            pltpu.VMEM((2, LANES, half_cols), BF16),
            pltpu.VMEM((hidden, width), BF16),
            pltpu.VMEM((hidden, width), BF16),
            pltpu.VMEM((2, hidden, half_cols), BF16),
            pltpu.VMEM(block, BF16),
            pltpu.VMEM(block, BF16),
            pltpu.VMEM(block, F32),
            pltpu.VMEM(block, BF16),
            pltpu.VMEM(block, BF16),
            pltpu.VMEM(block, BF16),
            pltpu.VMEM((groups, MAIN, message), BF16),
            pltpu.VMEM((2, groups, MAIN, message), BF16),
            pltpu.VMEM((all_rows, width), BF16),
            pltpu.VMEM((all_rows, half_cols), BF16),
            pltpu.VMEM((all_rows, half_cols), BF16),
            pltpu.VMEM((all_rows, half_cols), F32),
            pltpu.VMEM((groups, MAIN, message), BF16),
            pltpu.VMEM((groups, MAIN, message), BF16),
            pltpu.VMEM(block, BF16),
            pltpu.VMEM(block, BF16),
            dma((2,)),
            dma((2 * depth,)),
            dma((2 * depth,)),
            dma((2,)),
            dma((depth,)),
            dma((depth,)),
            dma((depth,)),
            dma((depth,)),
            dma((groups,)),
            dma((groups,)),
            dma((groups,)),
            dma((groups,)),
            dma((2,)),
            dma((groups,)),
            dma((groups,)),
            dma((depth,)),
            dma((depth,)),
        ],
        compiler_params=pltpu.CompilerParams(
            collective_id=0, has_side_effects=True, vmem_limit_bytes=48 * 2**20
        ),
        name="experts",
    )(
        mixed,
        tokens,
        routes.T,
        route_logits.T,
        row(ffn_gain),
        w_output,
        jnp.swapaxes(w_gate, 1, 2)[0],
        jnp.swapaxes(w_up, 1, 2)[0],
        w_down[0],
    )
    return (output, new_state)


def solution(mesh):
    return jax.shard_map(
        local,
        mesh=mesh,
        in_specs=(
            P("ep", None),
            P("ep", "tp", None, None),
            P("ep", None),
            P("ep", None),
            P(),
            P(None, "tp"),
            P(None, "tp"),
            P(None, "tp"),
            P(None, "tp"),
            P(None, "tp"),
            P("tp"),
            P("tp"),
            P("tp"),
            P("tp"),
            P("tp", None),
            P(),
            P("ep", None, "tp"),
            P("ep", None, "tp"),
            P("ep", "tp", None),
        ),
        out_specs=(P("ep", "tp"), P("ep", "tp", None, None)),
        check_vma=False,
    )
```

```python
import jax
import jax.numpy as jnp
from jax import lax
from jax.experimental import pallas as pl
from jax.experimental.pallas import tpu as pltpu
from jax.sharding import PartitionSpec as P

MESH = pl.DeviceIdType.MESH
RMS_EPS = 1e-06
GROUP_EPS = 0.00064
UNIT_EPS = 6.4e-05
F32 = jnp.float32
BF16 = jnp.bfloat16

LANES = 128
HALF = 64
SIDE = 4
CHUNKS = 4
PAIR = 8
MAIN = 8
REST = 4
GRANT = 67043328

NEAR = sorted(range(SIDE * SIDE), key=lambda o: sum(min(d, SIDE - d) for d in divmod(o, SIDE)))


def dot(a, b, contract=((1,), (0,))):
    return lax.dot_general(a, b, (contract, ((), ())), preferred_element_type=F32)


def mixer_kernel(
    tok_hbm,
    st_hbm,
    gain_hbm,
    w_recept,
    w_key,
    w_value,
    w_decay,
    w_rate,
    decay_hbm,
    rate_hbm,
    key_hbm,
    group_hbm,
    mixed_hbm,
    ns_hbm,
    mixed_ref,
    tok_v,
    mix_gain,
    vec_v,
    w_v,
    st_v,
    ns_v,
    rows_v,
    read_v,
    tok_sem,
    gain_sem,
    vec_sem,
    w_sem,
    st_sem,
    ns_sem,
):
    seqs = tok_v.shape[0]
    per = seqs // CHUNKS
    tok_copy = pltpu.make_async_copy(tok_hbm, tok_v, tok_sem)
    tok_copy.start()
    gain_copy = pltpu.make_async_copy(gain_hbm, mix_gain, gain_sem)
    gain_copy.start()
    for j, w_hbm in enumerate((w_recept, w_key, w_value, w_decay, w_rate)):
        pltpu.make_async_copy(w_hbm, w_v.at[:, pl.ds(j * LANES, LANES)], w_sem).start()
    for j, vec_hbm in enumerate((decay_hbm, rate_hbm, key_hbm, group_hbm)):
        pltpu.make_async_copy(vec_hbm, vec_v.at[j], vec_sem).start()

    def st_copy(i):
        part = pl.ds(i * per, per)
        return pltpu.make_async_copy(st_hbm.at[part], st_v.at[part], st_sem.at[i])

    def ns_copy(i):
        part = pl.ds(i * per, per)
        return pltpu.make_async_copy(ns_v.at[part], ns_hbm.at[part], ns_sem)

    lane = lax.broadcasted_iota(jnp.int32, (seqs, LANES), 1)

    def per_head(values):
        first = jnp.sum(jnp.where(lane < HALF, values, 0.0), axis=1, keepdims=True)
        second = jnp.sum(jnp.where(lane < HALF, 0.0, values), axis=1, keepdims=True)
        return jnp.where(lane < HALF, first, second)

    tok_copy.wait()
    for i in range(CHUNKS):
        st_copy(i).start()
    values = tok_v[...].astype(F32)
    scale = lax.rsqrt(jnp.mean(values * values, axis=1, keepdims=True) + RMS_EPS)
    gain_copy.wait()
    normed = (values * scale * mix_gain[...]).astype(BF16)
    pltpu.make_async_copy(w_v, w_v, w_sem).wait()
    pltpu.make_async_copy(vec_v, vec_v, vec_sem).wait()
    decay_base, rate_base, key_gain, group_gain = (vec_v[j] for j in range(4))
    projected = dot(normed, w_v[...]).astype(BF16).astype(F32)
    recept, key, value, decay_in, rate_in = (
        projected[:, j * LANES : (j + 1) * LANES] for j in range(5)
    )
    decay = jnp.exp(-(0.6065306597126334 * jax.nn.sigmoid(decay_in + decay_base)))
    rate = jax.nn.sigmoid(rate_in + rate_base)
    scaled = key * key_gain
    unit = scaled * lax.rsqrt(per_head(scaled * scaled) + UNIT_EPS)
    rows_v[0] = unit
    rows_v[1] = decay
    rows_v[2] = unit * rate
    rows_v[3] = key
    rows_v[4] = decay * recept
    rows_v[5] = value

    wide = 2 * LANES
    block_r = lax.broadcasted_iota(jnp.int32, (wide, wide), 0) // HALF
    block_c = lax.broadcasted_iota(jnp.int32, (wide, wide), 1) // HALF
    ones2 = (block_r == block_c).astype(BF16)
    ones1 = ones2[:LANES, :LANES]
    diag = (
        lax.broadcasted_iota(jnp.int32, (HALF, LANES), 0)
        == lax.broadcasted_iota(jnp.int32, (HALF, LANES), 1) % HALF
    )[None]

    def chunk(i, carry):
        st_copy(i).wait()
        for p in range(per // PAIR):
            part = pl.ds(i * per + p * PAIR, PAIR)
            old = jnp.concatenate([st_v[part, 0], st_v[part, 1]], axis=-1)
            unit_c, decay_c, take_c, key_c, seen_c, value_c = (
                rows_v[j, part][:, None, :] for j in range(6)
            )
            probe = (old * unit_c).astype(BF16).reshape(PAIR * HALF, LANES)
            spread = jnp.where(diag, value_c, 0.0).astype(BF16).reshape(PAIR * HALF, LANES)
            both = dot(jnp.concatenate([probe, spread], axis=1), ones2)
            seen = dot((old * seen_c).astype(BF16).reshape(PAIR * HALF, LANES), ones1)
            removed = both[:, :LANES].reshape(PAIR, HALF, LANES)
            value_b = both[:, LANES:].reshape(PAIR, HALF, LANES)
            new = old * decay_c - removed * take_c + value_b * key_c
            ns_v[part, 0] = new[..., :HALF]
            ns_v[part, 1] = new[..., HALF:]
            read_v[0, part, :] = jnp.sum(jnp.where(diag, removed, 0.0), axis=1)
            seen = jnp.where(diag, seen.reshape(PAIR, HALF, LANES), 0.0)
            read_v[1, part, :] = jnp.sum(seen, axis=1)
        ns_copy(i).start()
        return carry

    lax.fori_loop(0, CHUNKS, chunk, 0)
    readout = read_v[1] - read_v[0] * per_head(unit * rate * recept) + value * per_head(key * recept)
    centred = readout - per_head(readout) * (1.0 / HALF)
    spread = per_head(centred * centred) * (1.0 / HALF)
    mixed_ref[...] = (centred * lax.rsqrt(spread + GROUP_EPS) * group_gain).astype(BF16)
    mixed_copy = pltpu.make_async_copy(mixed_ref, mixed_hbm, tok_sem)
    mixed_copy.start()
    pltpu.make_async_copy(ns_v, ns_hbm, ns_sem).wait()
    mixed_copy.wait()


def expert_kernel(
    mixed_hbm,
    tok_hbm,
    routes_hbm,
    logits_hbm,
    gain_hbm,
    wo_hbm,
    wg_hbm,
    wu_hbm,
    wd_hbm,
    out_ref,
    mixed_ref,
    tok_ref,
    routes_ref,
    logits_ref,
    gain_ref,
    wo_v,
    wg_v,
    wu_v,
    wd_v,
    pair_send,
    pair_recv,
    own_v,
    rs_send,
    rs_recv,
    resid_v,
    disp_send,
    x_recv,
    gate_v,
    up_v,
    y_send,
    y_recv,
    ret_send,
    ret_recv,
    moe_send,
    moe_recv,
    in_sem,
    w_sem,
    send_sem,
    pair_sem,
    rs_sem,
    ag_sem,
    disp_sem,
    relay_sem,
    y_sem,
    ret_sem,
    moe_sem,
):
    depth = lax.axis_size("tp") // 2
    rows = tok_ref.shape[0]
    groups = SIDE * SIDE
    ep = lax.axis_index("ep")
    tp = lax.axis_index("tp")
    z, core = tp // 2, tp % 2
    y, x = ep // SIDE, ep % SIDE
    other = 1 - core

    def up_z(dz):
        return (z + dz) % depth

    def down_z(dz):
        return (z - dz + depth) % depth

    def along(dz):
        return (ep, up_z(dz) * 2 + core)

    def plane(o, sign):
        dy, dx = divmod(o, SIDE)
        to_y = (y + sign * dy + SIDE) % SIDE
        to_x = (x + sign * dx + SIDE) % SIDE
        return (to_y * SIDE + to_x, tp)

    partner = (ep, z * 2 + other)

    def send(src, dst, sender_sem, recv_sem, target):
        pltpu.make_async_remote_copy(
            src_ref=src,
            dst_ref=dst,
            send_sem=sender_sem,
            recv_sem=recv_sem,
            device_id=target,
            device_id_type=MESH,
        ).start()

    def take(ref, sem):
        pltpu.make_async_copy(ref, ref, sem).wait()

    def fetch(src, dst, sem):
        pltpu.make_async_copy(src, dst, sem).start()

    barrier = pltpu.get_barrier_semaphore()
    peers = [partner] + [along(dz) for dz in range(1, depth)]
    peers += [plane(o, 1) for o in range(1, groups)]
    for peer in peers:
        pl.semaphore_signal(barrier, inc=1, device_id=peer, device_id_type=MESH)

    fetch(mixed_hbm, mixed_ref, in_sem.at[0])
    for j in range(2 * depth):
        fetch(wo_hbm.at[:, pl.ds(j * LANES, LANES)], wo_v.at[j % 2, j // 2], in_sem.at[1])
    own_cols = pl.ds(pl.multiple_of(tp * LANES, LANES), LANES)
    fetch(routes_hbm, routes_ref, in_sem.at[2])
    fetch(logits_hbm, logits_ref, in_sem.at[3])
    fetch(tok_hbm.at[:, own_cols], tok_ref, in_sem.at[4])
    fetch(gain_hbm, gain_ref, in_sem.at[5])

    take(mixed_ref, in_sem.at[0])
    take(wo_v, in_sem.at[1])
    fetch(wg_hbm, wg_v, w_sem.at[0])
    fetch(wu_hbm, wu_v, w_sem.at[1])
    for j in range(2 * depth):
        fetch(wd_hbm.at[:, pl.ds(j * LANES, LANES)], wd_v.at[j % 2, j // 2], w_sem.at[2])

    mixed = mixed_ref[...]

    def wide(ref, side, blocks):
        return jnp.concatenate([ref[side, k] for k in blocks], axis=1)

    theirs = dot(mixed, wide(wo_v, other, range(depth))).astype(BF16)
    for k in range(depth):
        pair_send[k] = theirs[:, k * LANES : (k + 1) * LANES]
    pl.semaphore_wait(barrier, len(peers))
    send(pair_send, pair_recv, send_sem.at[0], pair_sem, partner)
    mine = dot(mixed, wide(wo_v, core, range(depth)))
    for k in range(depth):
        own_v[k] = mine[:, k * LANES : (k + 1) * LANES]
    take(pair_recv, pair_sem)

    far = sorted(range(1, depth), key=lambda dz: -min(dz, depth - dz))
    for dz in far:
        k = up_z(dz)
        rs_send[dz] = (own_v[k] + pair_recv[k].astype(F32)).astype(BF16)
        send(rs_send.at[dz], rs_recv.at[dz], send_sem.at[1], rs_sem, along(dz))
    total = own_v[z] + pair_recv[z].astype(F32)

    for j, ref in enumerate((routes_ref, logits_ref, tok_ref, gain_ref)):
        take(ref, in_sem.at[2 + j])
    row16 = lax.broadcasted_iota(jnp.int32, (groups, rows), 0)
    expert = (((y + (row16 >> 2)) & 3) << 2) | ((x + (row16 & 3)) & 3)
    first = (routes_ref[0:1, :] == expert).astype(BF16)
    second = (routes_ref[1:2, :] == expert).astype(BF16)
    before = (
        lax.broadcasted_iota(jnp.int32, (rows, rows), 0)
        < lax.broadcasted_iota(jnp.int32, (rows, rows), 1)
    ).astype(BF16)
    rank = dot(first + second, before).astype(BF16)
    slots = groups * MAIN
    expand = (
        (lax.broadcasted_iota(jnp.int32, (slots, groups), 0) // MAIN)
        == lax.broadcasted_iota(jnp.int32, (slots, groups), 1)
    ).astype(BF16)
    first_x = dot(expand, first)
    second_x = dot(expand, second)
    rank_x = dot(expand, rank).astype(jnp.int32)
    slot = lax.broadcasted_iota(jnp.int32, (slots, rows), 0) % MAIN
    named = (first_x + second_x) > 0.5
    pick_main = jnp.where(named & (rank_x == slot), 1.0, 0.0)
    pick_low = jnp.where(named & (rank_x == slot + MAIN) & (slot < REST), 1.0, 0.0)
    pick_high = jnp.where(named & (rank_x == slot + REST) & (slot >= REST), 1.0, 0.0)
    exp0 = jnp.exp(logits_ref[0:1, :])
    exp1 = jnp.exp(logits_ref[1:2, :])
    weight = (first_x * exp0 + second_x * exp1) / (exp0 + exp1)

    def split(table):
        turned = (table * weight).T
        top = turned.astype(BF16)
        return top, (turned - top.astype(F32)).astype(BF16)

    give_main, give_low, give_high = split(pick_main), split(pick_low), split(pick_high)
    pick_main, pick_low, pick_high = (t.astype(BF16) for t in (pick_main, pick_low, pick_high))

    take(rs_recv.at[pl.ds(1, depth - 1)], rs_sem)
    for dz in far:
        total = total + rs_recv[dz].astype(F32)
    own_resid = (tok_ref[...].astype(F32) + total).astype(BF16)
    resid_v[z] = own_resid

    ins = [(-j % depth, j + 1) for j in range(depth // 2)]
    pair_of = {dz: j for j, pair in enumerate(ins) for dz in pair}
    for dz in far:
        send(resid_v.at[z], resid_v.at[z], send_sem.at[2], ag_sem.at[pair_of[dz]], along(dz))
    two = 2 * LANES
    for j, (da, db) in enumerate(ins):
        if j:
            take(rs_recv.at[pl.ds(0, 2)], ag_sem.at[j])
        else:
            take(rs_recv.at[0], ag_sem.at[j])
        block_a, block_b = resid_v[down_z(da)], resid_v[down_z(db)]
        main = dot(pick_main, jnp.concatenate([block_a, block_b], axis=1)).astype(BF16)
        rest = (dot(pick_low, block_a) + dot(pick_high, block_b)).astype(BF16)
        disp_send[j, :, :, 0:two] = main.reshape(groups, MAIN, two)
        disp_send[j, :, :, two:] = rest.reshape(groups, MAIN, LANES)
        x_recv[core, j, 0] = disp_send[j, 0]
        for o in reversed(NEAR[1:]):
            src, dst = disp_send.at[j, o], x_recv.at[core, j, o]
            send(src, dst, send_sem.at[3], disp_sem.at[j], plane(o, 1))
    for j in range(len(ins)):
        take(x_recv.at[core, j, pl.ds(1, groups - 1)], disp_sem.at[j])
        block = x_recv.at[core, j]
        send(block, block, send_sem.at[4], relay_sem.at[j], partner)

    main_rows = groups * MAIN
    tile_row = lax.broadcasted_iota(jnp.int32, (groups // 2, MAIN, LANES), 1)
    upper = tile_row < REST
    squares = None
    for j, (da, db) in enumerate(ins):
        take(x_recv.at[other, j], relay_sem.at[j])
        if j == 0:
            take(wg_v, w_sem.at[0])
            take(wu_v, w_sem.at[1])
        mains, rests, gates, ups = [], [], [], []
        for p in range(2):
            got = x_recv[p, j].astype(F32)
            rest = got[:, :, two:].reshape(groups // 2, 2, MAIN, LANES)
            a, b = rest[:, 0], rest[:, 1]
            rest_a = jnp.where(upper, a, pltpu.roll(b, REST, 1)).reshape(-1, LANES)
            rest_b = jnp.where(upper, pltpu.roll(a, REST, 1), b).reshape(-1, LANES)
            for at, (dz, rest_d) in enumerate(((da, rest_a), (db, rest_b))):
                cols = pl.ds(pl.multiple_of((2 * down_z(dz) + p) * LANES, LANES), LANES)
                main = got[:, :, at * LANES : (at + 1) * LANES].reshape(main_rows, LANES)
                mains.append((main, gain_ref[:, cols]))
                rests.append((rest_d, gain_ref[:, cols]))
                gates.append(wg_v[:, cols])
                ups.append(wu_v[:, cols])
        parts = []
        for pieces in (mains, rests):
            squared = sum(jnp.sum(piece * piece, axis=1, keepdims=True) for piece, _ in pieces)
            scaled = jnp.concatenate([(piece * g).astype(BF16) for piece, g in pieces], axis=1)
            parts.append((squared, scaled))
        squared = jnp.concatenate([parts[0][0], parts[1][0]], axis=0)
        scaled = jnp.concatenate([parts[0][1], parts[1][1]], axis=0)
        gate = dot(scaled, jnp.concatenate(gates, axis=1), ((1,), (1,)))
        up = dot(scaled, jnp.concatenate(ups, axis=1), ((1,), (1,)))
        if j:
            squares = squares + squared
            gate = gate + gate_v[...]
            up = up + up_v[...]
        else:
            squares = squared
        if j < len(ins) - 1:
            gate_v[...] = gate
            up_v[...] = up
    scale = lax.rsqrt(squares * (1.0 / (2 * depth * LANES)) + RMS_EPS)
    gate = gate * scale
    hidden = (gate * jax.nn.sigmoid(gate) * (up * scale)).astype(BF16)

    take(wd_v, w_sem.at[2])
    outs = [(depth // 2 + j, depth // 2 - 1 - j) for j in range(depth // 2)]
    for j, pair in enumerate(outs):
        blocks = [up_z(dz) for dz in pair]
        y_send[j] = dot(hidden, wide(wd_v, other, blocks)).astype(BF16)
        send(y_send.at[j], y_recv.at[j], send_sem.at[5], y_sem.at[j], partner)
    for j, pair in enumerate(outs):
        blocks = [up_z(dz) for dz in pair]
        summed = dot(hidden, wide(wd_v, core, blocks))
        take(y_recv.at[j], y_sem.at[j])
        summed = summed + y_recv[j].astype(F32)
        ret_send[j, :, :, 0:two] = summed[:main_rows].astype(BF16).reshape(groups, MAIN, two)
        rest = summed[main_rows:].reshape(groups // 2, MAIN, two)
        rest_a, rest_b = rest[:, :, :LANES], rest[:, :, LANES:]
        even = jnp.where(upper, rest_a, pltpu.roll(rest_b, REST, 1)).astype(BF16)
        odd = jnp.where(upper, pltpu.roll(rest_a, REST, 1), rest_b).astype(BF16)
        for p in range(groups // 2):
            ret_send[j, 2 * p, :, two:] = even[p]
            ret_send[j, 2 * p + 1, :, two:] = odd[p]
        ret_recv[j, 0] = ret_send[j, 0]
        for o in reversed(NEAR[1:]):
            src, dst = ret_send.at[j, o], ret_recv.at[j, o]
            send(src, dst, send_sem.at[6], ret_sem.at[j], plane(o, -1))

    def give(tables, data):
        return dot(tables[0], data) + dot(tables[1], data)

    for j, (da, db) in enumerate(outs):
        take(ret_recv.at[j, pl.ds(1, groups - 1)], ret_sem.at[j])
        back = ret_recv[j]
        main = give(give_main, back[:, :, :two].reshape(slots, two))
        rest = back[:, :, two:].reshape(slots, LANES)
        for dz, moe in (
            (da, main[:, :LANES] + give(give_low, rest)),
            (db, main[:, LANES:] + give(give_high, rest)),
        ):
            if dz:
                moe_send[dz] = moe.astype(BF16)
                send(moe_send.at[dz], moe_recv.at[dz], send_sem.at[7], moe_sem, along(dz))
            else:
                total = own_resid.astype(F32) + moe
    take(moe_recv.at[pl.ds(1, depth - 1)], moe_sem)
    for dz in far:
        total = total + moe_recv[dz].astype(F32)
    out_ref[...] = total.astype(BF16)

    seven = pl.ds(1, depth - 1)
    take(pair_send, send_sem.at[0])
    take(rs_send.at[seven], send_sem.at[1])
    take(rs_send.at[seven], send_sem.at[2])
    take(disp_send.at[:, pl.ds(1, groups - 1)], send_sem.at[3])
    take(x_recv.at[core], send_sem.at[4])
    take(y_send, send_sem.at[5])
    take(ret_send.at[:, pl.ds(1, groups - 1)], send_sem.at[6])
    take(moe_send.at[seven], send_sem.at[7])


def local(
    tokens,
    state,
    routes,
    route_logits,
    mix_gain,
    w_recept,
    w_key,
    w_value,
    w_decay,
    w_rate,
    decay_base,
    rate_base,
    key_gain,
    group_gain,
    w_output,
    ffn_gain,
    w_gate,
    w_up,
    w_down,
):
    seqs, width = tokens.shape
    hidden = w_gate.shape[2]
    vmem = pl.BlockSpec(memory_space=pltpu.VMEM)
    anywhere = pl.BlockSpec(memory_space=pl.ANY)
    dma = pltpu.SemaphoreType.DMA

    def row(vector):
        return vector.reshape(1, -1)

    mixed, new_state = pl.pallas_call(
        mixer_kernel,
        out_shape=(
            jax.ShapeDtypeStruct((seqs, LANES), BF16),
            jax.ShapeDtypeStruct(state.shape, F32),
        ),
        in_specs=[anywhere] * 12,
        out_specs=(anywhere, anywhere),
        scratch_shapes=[
            pltpu.VMEM((seqs, LANES), BF16),
            pltpu.VMEM((seqs, width), BF16),
            pltpu.VMEM((1, width), F32),
            pltpu.VMEM((4, 1, LANES), F32),
            pltpu.VMEM((width, 5 * LANES), BF16),
            pltpu.VMEM(state.shape, F32),
            pltpu.VMEM(state.shape, F32),
            pltpu.VMEM((6, seqs, LANES), F32),
            pltpu.VMEM((2, seqs, LANES), F32),
            dma(()),
            dma(()),
            dma(()),
            dma(()),
            dma((CHUNKS,)),
            dma(()),
        ],
        compiler_params=pltpu.CompilerParams(vmem_limit_bytes=GRANT),
        name="mixer",
    )(
        tokens,
        state,
        row(mix_gain),
        w_recept,
        w_key,
        w_value,
        w_decay,
        w_rate,
        row(decay_base),
        row(rate_base),
        row(key_gain),
        row(group_gain),
    )

    depth = lax.axis_size("tp") // 2
    groups = SIDE * SIDE
    pairs = depth // 2
    message = (pairs, groups, MAIN, 3 * LANES)
    all_rows = groups * (MAIN + REST)
    block = (depth, seqs, LANES)
    output = pl.pallas_call(
        expert_kernel,
        out_shape=jax.ShapeDtypeStruct((seqs, LANES), BF16),
        in_specs=[anywhere] * 9,
        out_specs=vmem,
        scratch_shapes=[
            pltpu.VMEM((seqs, LANES), BF16),
            pltpu.VMEM((seqs, LANES), BF16),
            pltpu.VMEM(routes.shape[::-1], jnp.int32),
            pltpu.VMEM(routes.shape[::-1], F32),
            pltpu.VMEM((1, width), F32),
            pltpu.VMEM((2, depth, LANES, LANES), BF16),
            pltpu.VMEM((hidden, width), BF16),
            pltpu.VMEM((hidden, width), BF16),
            pltpu.VMEM((2, depth, hidden, LANES), BF16),
            pltpu.VMEM(block, BF16),
            pltpu.VMEM(block, BF16),
            pltpu.VMEM(block, F32),
            pltpu.VMEM(block, BF16),
            pltpu.VMEM(block, BF16),
            pltpu.VMEM(block, BF16),
            pltpu.VMEM(message, BF16),
            pltpu.VMEM((2,) + message, BF16),
            pltpu.VMEM((all_rows, hidden), F32),
            pltpu.VMEM((all_rows, hidden), F32),
            pltpu.VMEM((pairs, all_rows, 2 * LANES), BF16),
            pltpu.VMEM((pairs, all_rows, 2 * LANES), BF16),
            pltpu.VMEM(message, BF16),
            pltpu.VMEM(message, BF16),
            pltpu.VMEM(block, BF16),
            pltpu.VMEM(block, BF16),
            dma((6,)),
            dma((3,)),
            dma((8,)),
            dma(()),
            dma(()),
            dma((pairs,)),
            dma((pairs,)),
            dma((pairs,)),
            dma((pairs,)),
            dma((pairs,)),
            dma(()),
        ],
        compiler_params=pltpu.CompilerParams(
            collective_id=0, has_side_effects=True, vmem_limit_bytes=GRANT
        ),
        name="experts",
    )(
        mixed,
        tokens,
        routes.T,
        route_logits.T,
        row(ffn_gain),
        w_output,
        jnp.swapaxes(w_gate, 1, 2)[0],
        jnp.swapaxes(w_up, 1, 2)[0],
        w_down[0],
    )
    return (output, new_state)


def solution(mesh):
    return jax.shard_map(
        local,
        mesh=mesh,
        in_specs=(
            P("ep", None),
            P("ep", "tp", None, None),
            P("ep", None),
            P("ep", None),
            P(),
            P(None, "tp"),
            P(None, "tp"),
            P(None, "tp"),
            P(None, "tp"),
            P(None, "tp"),
            P("tp"),
            P("tp"),
            P("tp"),
            P("tp"),
            P("tp", None),
            P(),
            P("ep", None, "tp"),
            P("ep", None, "tp"),
            P("ep", "tp", None),
        ),
        out_specs=(P("ep", "tp"), P("ep", "tp", None, None)),
        check_vma=False,
    )
```

```python
import jax
import jax.numpy as jnp
from jax import lax
from jax.experimental import pallas as pl
from jax.experimental.pallas import tpu as pltpu
from jax.sharding import PartitionSpec as P

MESH = pl.DeviceIdType.MESH
RMS_EPS = 1e-06
GROUP_EPS = 0.00064
UNIT_EPS = 6.4e-05
F32 = jnp.float32
BF16 = jnp.bfloat16

LANES = 128
HALF = 64
SIDE = 4
CHUNKS = 4
PAIR = 8
PIECES = 8
MAIN = 8
REST = 4
GRANT = 67043328

NEAR = sorted(range(SIDE * SIDE), key=lambda o: sum(min(d, SIDE - d) for d in divmod(o, SIDE)))


def dot(a, b, contract=((1,), (0,))):
    return lax.dot_general(a, b, (contract, ((), ())), preferred_element_type=F32)


def mixer(refs):
    (tok_hbm, st_hbm, gain_hbm, w_hbms, vec_hbms, ns_hbm) = refs[:6]
    (tok_v, gain_v, vec_v, w_v, st_v, ns_v, rows_v, read_v) = refs[6:14]
    (tok_sem, gain_sem, vec_sem, w_sem, st_sem, ns_sem) = refs[14:]
    seqs = tok_v.shape[0]
    per = seqs // CHUNKS
    tok_copy = pltpu.make_async_copy(tok_hbm, tok_v, tok_sem)
    tok_copy.start()
    gain_copy = pltpu.make_async_copy(gain_hbm, gain_v, gain_sem)
    gain_copy.start()
    for j, w_hbm in enumerate(w_hbms):
        pltpu.make_async_copy(w_hbm, w_v.at[:, pl.ds(j * LANES, LANES)], w_sem).start()
    for j, vec_hbm in enumerate(vec_hbms):
        pltpu.make_async_copy(vec_hbm, vec_v.at[j], vec_sem).start()

    def st_copy(i):
        part = pl.ds(i * per, per)
        return pltpu.make_async_copy(st_hbm.at[part], st_v.at[part], st_sem.at[i])

    def ns_copy(i):
        part = pl.ds(i * per, per)
        return pltpu.make_async_copy(ns_v.at[part], ns_hbm.at[part], ns_sem)

    lane = lax.broadcasted_iota(jnp.int32, (seqs, LANES), 1)

    def per_head(values):
        first = jnp.sum(jnp.where(lane < HALF, values, 0.0), axis=1, keepdims=True)
        second = jnp.sum(jnp.where(lane < HALF, 0.0, values), axis=1, keepdims=True)
        return jnp.where(lane < HALF, first, second)

    wide = 2 * LANES
    block_r = lax.broadcasted_iota(jnp.int32, (wide, wide), 0) // HALF
    block_c = lax.broadcasted_iota(jnp.int32, (wide, wide), 1) // HALF
    diag = (
        lax.broadcasted_iota(jnp.int32, (HALF, LANES), 0)
        == lax.broadcasted_iota(jnp.int32, (HALF, LANES), 1) % HALF
    )[None]

    def old_state(part):
        return jnp.concatenate([st_v[part, 0], st_v[part, 1]], axis=-1)

    def row_of(j, part):
        return rows_v[j, part][:, None, :]

    def flat(values):
        return values.astype(BF16).reshape(PAIR * HALF, LANES)

    def head_sums(left, right):
        ones = (block_r == block_c).astype(BF16)
        both = dot(jnp.concatenate([flat(left), flat(right)], axis=1), ones)
        return (
            both[:, :LANES].reshape(PAIR, HALF, LANES),
            both[:, LANES:].reshape(PAIR, HALF, LANES),
        )

    def mixed_rows(fetch_rest):
        tok_copy.wait()
        for i in range(CHUNKS):
            st_copy(i).start()
        fetch_rest()
        values = tok_v[...].astype(F32)
        scale = lax.rsqrt(jnp.mean(values * values, axis=1, keepdims=True) + RMS_EPS)
        gain_copy.wait()
        normed = (values * scale * gain_v[...]).astype(BF16)
        pltpu.make_async_copy(w_v, w_v, w_sem).wait()
        pltpu.make_async_copy(vec_v, vec_v, vec_sem).wait()
        decay_base, rate_base, key_gain, group_gain = (vec_v[j] for j in range(4))
        projected = dot(normed, w_v[...]).astype(BF16).astype(F32)
        recept, key, value, decay_in, rate_in = (
            projected[:, j * LANES : (j + 1) * LANES] for j in range(5)
        )
        decay = jnp.exp(-(0.6065306597126334 * jax.nn.sigmoid(decay_in + decay_base)))
        rate = jax.nn.sigmoid(rate_in + rate_base)
        scaled = key * key_gain
        unit = scaled * lax.rsqrt(per_head(scaled * scaled) + UNIT_EPS)
        rows_v[0] = unit
        rows_v[1] = decay
        rows_v[2] = unit * rate
        rows_v[3] = key
        rows_v[4] = decay * recept
        rows_v[5] = value

        def look(i, carry):
            st_copy(i).wait()
            for p in range(per // PAIR):
                part = pl.ds(i * per + p * PAIR, PAIR)
                old = old_state(part)
                removed, seen = head_sums(old * row_of(0, part), old * row_of(4, part))
                read_v[0, part, :] = jnp.sum(jnp.where(diag, removed, 0.0), axis=1)
                read_v[1, part, :] = jnp.sum(jnp.where(diag, seen, 0.0), axis=1)
            return carry

        lax.fori_loop(0, CHUNKS, look, 0)
        taken = read_v[0] * per_head(unit * rate * recept)
        readout = read_v[1] - taken + value * per_head(key * recept)
        centred = readout - per_head(readout) * (1.0 / HALF)
        spread = per_head(centred * centred) * (1.0 / HALF)
        return (centred * lax.rsqrt(spread + GROUP_EPS) * group_gain).astype(BF16)

    def update():
        def chunk(i, carry):
            for p in range(per // PAIR):
                part = pl.ds(i * per + p * PAIR, PAIR)
                old = old_state(part)
                spread = jnp.where(diag, row_of(5, part), 0.0)
                removed, value = head_sums(old * row_of(0, part), spread)
                new = old * row_of(1, part) - removed * row_of(2, part) + value * row_of(3, part)
                ns_v[part] = new
            ns_copy(i).start()
            return carry

        lax.fori_loop(0, CHUNKS, chunk, 0)

    def finish():
        pltpu.make_async_copy(ns_v, ns_hbm, ns_sem).wait()

    return mixed_rows, update, finish


def layer_kernel(
    tok_hbm,
    st_hbm,
    mix_gain_hbm,
    wr_hbm,
    wk_hbm,
    wv_hbm,
    wdec_hbm,
    wrate_hbm,
    decay_hbm,
    rate_hbm,
    key_hbm,
    group_hbm,
    routes_hbm,
    logits_hbm,
    gain_hbm,
    wo_hbm,
    wg_hbm,
    wu_hbm,
    wd_hbm,
    out_ref,
    ns_hbm,
    mtok_v,
    mgain_v,
    vec_v,
    w_v,
    st_v,
    ns_v,
    rows_v,
    read_v,
    tok_ref,
    routes_ref,
    logits_ref,
    gain_ref,
    wo_v,
    wg_v,
    wu_v,
    wd_v,
    pair_send,
    pair_recv,
    own_v,
    rs_send,
    rs_recv,
    resid_v,
    disp_send,
    x_recv,
    gate_v,
    up_v,
    y_send,
    y_recv,
    ret_send,
    ret_recv,
    moe_send,
    moe_recv,
    mtok_sem,
    mgain_sem,
    vec_sem,
    mw_sem,
    st_sem,
    ns_sem,
    in_sem,
    w_sem,
    send_sem,
    pair_sem,
    rs_sem,
    ag_sem,
    disp_sem,
    relay_sem,
    y_sem,
    ret_sem,
    moe_sem,
):
    depth = lax.axis_size("tp") // 2
    rows = tok_ref.shape[0]
    groups = SIDE * SIDE
    ep = lax.axis_index("ep")
    tp = lax.axis_index("tp")
    z, core = tp // 2, tp % 2
    y, x = ep // SIDE, ep % SIDE
    other = 1 - core

    def up_z(dz):
        return (z + dz) % depth

    def down_z(dz):
        return (z - dz + depth) % depth

    def along(dz):
        return (ep, up_z(dz) * 2 + core)

    def plane(o, sign):
        dy, dx = divmod(o, SIDE)
        to_y = (y + sign * dy + SIDE) % SIDE
        to_x = (x + sign * dx + SIDE) % SIDE
        return (to_y * SIDE + to_x, tp)

    partner = (ep, z * 2 + other)

    def send(src, dst, sender_sem, recv_sem, target):
        pltpu.make_async_remote_copy(
            src_ref=src,
            dst_ref=dst,
            send_sem=sender_sem,
            recv_sem=recv_sem,
            device_id=target,
            device_id_type=MESH,
        ).start()

    def take(ref, sem):
        pltpu.make_async_copy(ref, ref, sem).wait()

    def fetch(src, dst, sem):
        pltpu.make_async_copy(src, dst, sem).start()

    mixed_rows, update, finish = mixer(
        (
            tok_hbm,
            st_hbm,
            mix_gain_hbm,
            (wr_hbm, wk_hbm, wv_hbm, wdec_hbm, wrate_hbm),
            (decay_hbm, rate_hbm, key_hbm, group_hbm),
            ns_hbm,
            mtok_v,
            mgain_v,
            vec_v,
            w_v,
            st_v,
            ns_v,
            rows_v,
            read_v,
            mtok_sem,
            mgain_sem,
            vec_sem,
            mw_sem,
            st_sem,
            ns_sem,
        )
    )
    barrier = pltpu.get_barrier_semaphore()
    peers = [partner] + [along(dz) for dz in range(1, depth)]
    peers += [plane(o, 1) for o in range(1, groups)]
    for peer in peers:
        pl.semaphore_signal(barrier, inc=1, device_id=peer, device_id_type=MESH)

    def fetch_rest():
        for j in range(2 * depth):
            fetch(wo_hbm.at[:, pl.ds(j * LANES, LANES)], wo_v.at[j % 2, j // 2], in_sem.at[0])
        own_cols = pl.ds(pl.multiple_of(tp * LANES, LANES), LANES)
        fetch(routes_hbm, routes_ref, in_sem.at[1])
        fetch(logits_hbm, logits_ref, in_sem.at[2])
        fetch(tok_hbm.at[:, own_cols], tok_ref, in_sem.at[3])
        fetch(gain_hbm, gain_ref, in_sem.at[4])

    mixed = mixed_rows(fetch_rest)
    take(wo_v, in_sem.at[0])

    def wide(ref, side, blocks):
        return jnp.concatenate([ref[side, k] for k in blocks], axis=1)

    theirs = dot(mixed, wide(wo_v, other, range(depth))).astype(BF16)
    for k in range(depth):
        pair_send[k] = theirs[:, k * LANES : (k + 1) * LANES]
    pl.semaphore_wait(barrier, len(peers))
    send(pair_send, pair_recv, send_sem.at[0], pair_sem, partner)
    fetch(wg_hbm, wg_v, w_sem.at[0])
    fetch(wu_hbm, wu_v, w_sem.at[1])
    for j in range(2 * depth):
        fetch(wd_hbm.at[:, pl.ds(j * LANES, LANES)], wd_v.at[j % 2, j // 2], w_sem.at[2])
    mine = dot(mixed, wide(wo_v, core, range(depth)))
    for k in range(depth):
        own_v[k] = mine[:, k * LANES : (k + 1) * LANES]
    take(pair_recv, pair_sem)

    far = sorted(range(1, depth), key=lambda dz: -min(dz, depth - dz))
    for dz in far:
        k = up_z(dz)
        rs_send[dz] = (own_v[k] + pair_recv[k].astype(F32)).astype(BF16)
        send(rs_send.at[dz], rs_recv.at[dz], send_sem.at[1], rs_sem, along(dz))
    total = own_v[z] + pair_recv[z].astype(F32)

    for j, ref in enumerate((routes_ref, logits_ref, tok_ref, gain_ref)):
        take(ref, in_sem.at[1 + j])
    row16 = lax.broadcasted_iota(jnp.int32, (groups, rows), 0)
    expert = (((y + (row16 >> 2)) & 3) << 2) | ((x + (row16 & 3)) & 3)
    first = (routes_ref[0:1, :] == expert).astype(BF16)
    second = (routes_ref[1:2, :] == expert).astype(BF16)
    before = (
        lax.broadcasted_iota(jnp.int32, (rows, rows), 0)
        < lax.broadcasted_iota(jnp.int32, (rows, rows), 1)
    ).astype(BF16)
    rank = dot(first + second, before).astype(BF16)
    slots = groups * MAIN
    expand = (
        (lax.broadcasted_iota(jnp.int32, (slots, groups), 0) // MAIN)
        == lax.broadcasted_iota(jnp.int32, (slots, groups), 1)
    ).astype(BF16)
    first_x = dot(expand, first)
    second_x = dot(expand, second)
    rank_x = dot(expand, rank).astype(jnp.int32)
    slot = lax.broadcasted_iota(jnp.int32, (slots, rows), 0) % MAIN
    named = (first_x + second_x) > 0.5
    pick_main = jnp.where(named & (rank_x == slot), 1.0, 0.0)
    pick_low = jnp.where(named & (rank_x == slot + MAIN) & (slot < REST), 1.0, 0.0)
    pick_high = jnp.where(named & (rank_x == slot + REST) & (slot >= REST), 1.0, 0.0)
    exp0 = jnp.exp(logits_ref[0:1, :])
    exp1 = jnp.exp(logits_ref[1:2, :])
    weight = (first_x * exp0 + second_x * exp1) / (exp0 + exp1)

    def split(table):
        turned = (table * weight).T
        top = turned.astype(BF16)
        return top, (turned - top.astype(F32)).astype(BF16)

    give_main, give_low, give_high = split(pick_main), split(pick_low), split(pick_high)
    pick_main, pick_low, pick_high = (t.astype(BF16) for t in (pick_main, pick_low, pick_high))

    update()
    take(rs_recv.at[pl.ds(1, depth - 1)], rs_sem)
    for dz in far:
        total = total + rs_recv[dz].astype(F32)
    own_resid = (tok_ref[...].astype(F32) + total).astype(BF16)
    resid_v[z] = own_resid

    ins = [(-j % depth, j + 1) for j in range(depth // 2)]
    pair_of = {dz: j for j, pair in enumerate(ins) for dz in pair}
    for dz in reversed(far):
        send(resid_v.at[z], resid_v.at[z], send_sem.at[2], ag_sem.at[pair_of[dz]], along(dz))
    two = 2 * LANES
    for j, (da, db) in enumerate(ins):
        if j:
            take(rs_recv.at[pl.ds(0, 2)], ag_sem.at[j])
        else:
            take(rs_recv.at[0], ag_sem.at[j])
        block_a, block_b = resid_v[down_z(da)], resid_v[down_z(db)]
        main = dot(pick_main, jnp.concatenate([block_a, block_b], axis=1)).astype(BF16)
        rest = (dot(pick_low, block_a) + dot(pick_high, block_b)).astype(BF16)
        disp_send[j, :, :, 0:two] = main.reshape(groups, MAIN, two)
        disp_send[j, :, :, two:] = rest.reshape(groups, MAIN, LANES)
        x_recv[core, j, 0] = disp_send[j, 0]
        for o in reversed(NEAR[1:]):
            src, dst = disp_send.at[j, o], x_recv.at[core, j, o]
            send(src, dst, send_sem.at[3], disp_sem.at[j], plane(o, 1))
    for j in range(len(ins)):
        take(x_recv.at[core, j, pl.ds(1, groups - 1)], disp_sem.at[j])
        block = x_recv.at[core, j]
        send(block, block, send_sem.at[4], relay_sem.at[j], partner)

    main_rows = groups * MAIN
    tile_row = lax.broadcasted_iota(jnp.int32, (groups // 2, MAIN, LANES), 1)
    upper = tile_row < REST
    squares = None
    for j, (da, db) in enumerate(ins):
        take(x_recv.at[other, j], relay_sem.at[j])
        if j == 0:
            take(wg_v, w_sem.at[0])
            take(wu_v, w_sem.at[1])
        mains, rests, gates, ups = [], [], [], []
        for p in range(2):
            got = x_recv[p, j].astype(F32)
            rest = got[:, :, two:].reshape(groups // 2, 2, MAIN, LANES)
            a, b = rest[:, 0], rest[:, 1]
            rest_a = jnp.where(upper, a, pltpu.roll(b, REST, 1)).reshape(-1, LANES)
            rest_b = jnp.where(upper, pltpu.roll(a, REST, 1), b).reshape(-1, LANES)
            for at, (dz, rest_d) in enumerate(((da, rest_a), (db, rest_b))):
                cols = pl.ds(pl.multiple_of((2 * down_z(dz) + p) * LANES, LANES), LANES)
                main = got[:, :, at * LANES : (at + 1) * LANES].reshape(main_rows, LANES)
                mains.append((main, gain_ref[:, cols]))
                rests.append((rest_d, gain_ref[:, cols]))
                gates.append(wg_v[:, cols])
                ups.append(wu_v[:, cols])
        parts = []
        for pieces in (mains, rests):
            squared = sum(jnp.sum(piece * piece, axis=1, keepdims=True) for piece, _ in pieces)
            scaled = jnp.concatenate([(piece * g).astype(BF16) for piece, g in pieces], axis=1)
            parts.append((squared, scaled))
        squared = jnp.concatenate([parts[0][0], parts[1][0]], axis=0)
        scaled = jnp.concatenate([parts[0][1], parts[1][1]], axis=0)
        gate = dot(scaled, jnp.concatenate(gates, axis=1), ((1,), (1,)))
        up = dot(scaled, jnp.concatenate(ups, axis=1), ((1,), (1,)))
        if j:
            squares = squares + squared
            gate = gate + gate_v[...]
            up = up + up_v[...]
        else:
            squares = squared
        if j < len(ins) - 1:
            gate_v[...] = gate
            up_v[...] = up
    scale = lax.rsqrt(squares * (1.0 / (2 * depth * LANES)) + RMS_EPS)
    gate = gate * scale
    hidden = (gate * jax.nn.sigmoid(gate) * (up * scale)).astype(BF16)

    take(wd_v, w_sem.at[2])
    outs = [(depth // 2 + j, depth // 2 - 1 - j) for j in range(depth // 2)]
    for j, pair in enumerate(outs):
        blocks = [up_z(dz) for dz in pair]
        y_send[j] = dot(hidden, wide(wd_v, other, blocks)).astype(BF16)
        send(y_send.at[j], y_recv.at[j], send_sem.at[5], y_sem.at[j], partner)
    for j, pair in enumerate(outs):
        blocks = [up_z(dz) for dz in pair]
        summed = dot(hidden, wide(wd_v, core, blocks))
        take(y_recv.at[j], y_sem.at[j])
        summed = summed + y_recv[j].astype(F32)
        ret_send[j, :, :, 0:two] = summed[:main_rows].astype(BF16).reshape(groups, MAIN, two)
        rest = summed[main_rows:].reshape(groups // 2, MAIN, two)
        rest_a, rest_b = rest[:, :, :LANES], rest[:, :, LANES:]
        even = jnp.where(upper, rest_a, pltpu.roll(rest_b, REST, 1)).astype(BF16)
        odd = jnp.where(upper, pltpu.roll(rest_a, REST, 1), rest_b).astype(BF16)
        for p in range(groups // 2):
            ret_send[j, 2 * p, :, two:] = even[p]
            ret_send[j, 2 * p + 1, :, two:] = odd[p]
        ret_recv[j, 0] = ret_send[j, 0]
        for o in reversed(NEAR[1:]):
            src, dst = ret_send.at[j, o], ret_recv.at[j, o]
            send(src, dst, send_sem.at[6], ret_sem.at[j], plane(o, -1))

    def give(tables, data):
        return dot(tables[0], data) + dot(tables[1], data)

    for j, (da, db) in enumerate(outs):
        take(ret_recv.at[j, pl.ds(1, groups - 1)], ret_sem.at[j])
        back = ret_recv[j]
        main = give(give_main, back[:, :, :two].reshape(slots, two))
        rest = back[:, :, two:].reshape(slots, LANES)
        for dz, moe in (
            (da, main[:, :LANES] + give(give_low, rest)),
            (db, main[:, LANES:] + give(give_high, rest)),
        ):
            if dz:
                moe_send[dz] = moe.astype(BF16)
                send(moe_send.at[dz], moe_recv.at[dz], send_sem.at[7], moe_sem, along(dz))
            else:
                total = own_resid.astype(F32) + moe
    take(moe_recv.at[pl.ds(1, depth - 1)], moe_sem)
    for dz in far:
        total = total + moe_recv[dz].astype(F32)
    out_ref[...] = total.astype(BF16)

    finish()
    seven = pl.ds(1, depth - 1)
    take(pair_send, send_sem.at[0])
    take(rs_send.at[seven], send_sem.at[1])
    take(rs_send.at[seven], send_sem.at[2])
    take(disp_send.at[:, pl.ds(1, groups - 1)], send_sem.at[3])
    take(x_recv.at[core], send_sem.at[4])
    take(y_send, send_sem.at[5])
    take(ret_send.at[:, pl.ds(1, groups - 1)], send_sem.at[6])
    take(moe_send.at[seven], send_sem.at[7])


def unpack_kernel(
    out_hbm, packed_hbm, copy_hbm, state_hbm, out_v, packed_v, state_v, out_sem, in_sem, st_sem
):
    per = packed_v.shape[0] // PIECES

    def piece(i):
        part = pl.ds(i * per, per)
        return pltpu.make_async_copy(packed_hbm.at[part], packed_v.at[part], in_sem.at[i])

    for i in range(PIECES):
        piece(i).start()
    take_out = pltpu.make_async_copy(out_hbm, out_v, out_sem.at[0])
    take_out.start()
    give_out = pltpu.make_async_copy(out_v, copy_hbm, out_sem.at[1])
    for i in range(PIECES):
        part = pl.ds(i * per, per)
        piece(i).wait()
        both = packed_v[part]
        state_v[part, 0] = both[..., :HALF]
        state_v[part, 1] = both[..., HALF:]
        pltpu.make_async_copy(state_v.at[part], state_hbm.at[part], st_sem).start()
        if i == 0:
            take_out.wait()
            give_out.start()
    give_out.wait()
    pltpu.make_async_copy(state_v, state_hbm, st_sem).wait()


def local(
    tokens,
    state,
    routes,
    route_logits,
    mix_gain,
    w_recept,
    w_key,
    w_value,
    w_decay,
    w_rate,
    decay_base,
    rate_base,
    key_gain,
    group_gain,
    w_output,
    ffn_gain,
    w_gate,
    w_up,
    w_down,
):
    seqs, width = tokens.shape
    hidden = w_gate.shape[2]
    vmem = pl.BlockSpec(memory_space=pltpu.VMEM)
    anywhere = pl.BlockSpec(memory_space=pl.ANY)
    dma = pltpu.SemaphoreType.DMA

    def row(vector):
        return vector.reshape(1, -1)

    depth = lax.axis_size("tp") // 2
    groups = SIDE * SIDE
    pairs = depth // 2
    message = (pairs, groups, MAIN, 3 * LANES)
    all_rows = groups * (MAIN + REST)
    block = (depth, seqs, LANES)
    packed = (seqs, state.shape[2], LANES)
    output, new_state = pl.pallas_call(
        layer_kernel,
        out_shape=(
            jax.ShapeDtypeStruct((seqs, LANES), BF16),
            jax.ShapeDtypeStruct(packed, F32),
        ),
        in_specs=[anywhere] * 19,
        out_specs=(vmem, anywhere),
        scratch_shapes=[
            pltpu.VMEM((seqs, width), BF16),
            pltpu.VMEM((1, width), F32),
            pltpu.VMEM((4, 1, LANES), F32),
            pltpu.VMEM((width, 5 * LANES), BF16),
            pltpu.VMEM(state.shape, F32),
            pltpu.VMEM(packed, F32),
            pltpu.VMEM((6, seqs, LANES), F32),
            pltpu.VMEM((2, seqs, LANES), F32),
            pltpu.VMEM((seqs, LANES), BF16),
            pltpu.VMEM(routes.shape[::-1], jnp.int32),
            pltpu.VMEM(routes.shape[::-1], F32),
            pltpu.VMEM((1, width), F32),
            pltpu.VMEM((2, depth, LANES, LANES), BF16),
            pltpu.VMEM((hidden, width), BF16),
            pltpu.VMEM((hidden, width), BF16),
            pltpu.VMEM((2, depth, hidden, LANES), BF16),
            pltpu.VMEM(block, BF16),
            pltpu.VMEM(block, BF16),
            pltpu.VMEM(block, F32),
            pltpu.VMEM(block, BF16),
            pltpu.VMEM(block, BF16),
            pltpu.VMEM(block, BF16),
            pltpu.VMEM(message, BF16),
            pltpu.VMEM((2,) + message, BF16),
            pltpu.VMEM((all_rows, hidden), F32),
            pltpu.VMEM((all_rows, hidden), F32),
            pltpu.VMEM((pairs, all_rows, 2 * LANES), BF16),
            pltpu.VMEM((pairs, all_rows, 2 * LANES), BF16),
            pltpu.VMEM(message, BF16),
            pltpu.VMEM(message, BF16),
            pltpu.VMEM(block, BF16),
            pltpu.VMEM(block, BF16),
            dma(()),
            dma(()),
            dma(()),
            dma(()),
            dma((CHUNKS,)),
            dma(()),
            dma((5,)),
            dma((3,)),
            dma((8,)),
            dma(()),
            dma(()),
            dma((pairs,)),
            dma((pairs,)),
            dma((pairs,)),
            dma((pairs,)),
            dma((pairs,)),
            dma(()),
        ],
        compiler_params=pltpu.CompilerParams(
            collective_id=0, has_side_effects=True, vmem_limit_bytes=GRANT
        ),
        name="layer",
    )(
        tokens,
        state,
        row(mix_gain),
        w_recept,
        w_key,
        w_value,
        w_decay,
        w_rate,
        row(decay_base),
        row(rate_base),
        row(key_gain),
        row(group_gain),
        routes.T,
        route_logits.T,
        row(ffn_gain),
        w_output,
        jnp.swapaxes(w_gate, 1, 2)[0],
        jnp.swapaxes(w_up, 1, 2)[0],
        w_down[0],
    )
    return pl.pallas_call(
        unpack_kernel,
        out_shape=(
            jax.ShapeDtypeStruct((seqs, LANES), BF16),
            jax.ShapeDtypeStruct(state.shape, F32),
        ),
        in_specs=[anywhere] * 2,
        out_specs=(anywhere, anywhere),
        scratch_shapes=[
            pltpu.VMEM((seqs, LANES), BF16),
            pltpu.VMEM(packed, F32),
            pltpu.VMEM(state.shape, F32),
            dma((2,)),
            dma((PIECES,)),
            dma(()),
        ],
        compiler_params=pltpu.CompilerParams(vmem_limit_bytes=GRANT),
        name="unpack",
    )(output, new_state)


def solution(mesh):
    return jax.shard_map(
        local,
        mesh=mesh,
        in_specs=(
            P("ep", None),
            P("ep", "tp", None, None),
            P("ep", None),
            P("ep", None),
            P(),
            P(None, "tp"),
            P(None, "tp"),
            P(None, "tp"),
            P(None, "tp"),
            P(None, "tp"),
            P("tp"),
            P("tp"),
            P("tp"),
            P("tp"),
            P("tp", None),
            P(),
            P("ep", None, "tp"),
            P("ep", None, "tp"),
            P("ep", "tp", None),
        ),
        out_specs=(P("ep", "tp"), P("ep", "tp", None, None)),
        check_vma=False,
    )
```

```python
import jax
import jax.numpy as jnp
from jax import lax
from jax.experimental import pallas as pl
from jax.experimental.pallas import tpu as pltpu
from jax.sharding import PartitionSpec as P

MESH = pl.DeviceIdType.MESH
RMS_EPS = 1e-06
GROUP_EPS = 0.00064
UNIT_EPS = 6.4e-05
F32 = jnp.float32
BF16 = jnp.bfloat16

LANES = 128
HALF = 64
SIDE = 4
CHUNKS = 4
PAIR = 8
PIECES = 8
MAIN = 8
REST = 4
GRANT = 67043328

NEAR = sorted(range(SIDE * SIDE), key=lambda o: sum(min(d, SIDE - d) for d in divmod(o, SIDE)))


def dot(a, b, contract=((1,), (0,))):
    return lax.dot_general(a, b, (contract, ((), ())), preferred_element_type=F32)


def mixer(refs):
    (tok_hbm, st_hbm, gain_hbm, w_hbms, vec_hbms, ns_hbm) = refs[:6]
    (tok_v, gain_v, vec_v, w_v, st_v, ns_v, rows_v, read_v) = refs[6:14]
    (tok_sem, gain_sem, vec_sem, w_sem, st_sem, ns_sem) = refs[14:]
    seqs = tok_v.shape[0]
    per = seqs // CHUNKS
    tok_copy = pltpu.make_async_copy(tok_hbm, tok_v, tok_sem)
    tok_copy.start()
    gain_copy = pltpu.make_async_copy(gain_hbm, gain_v, gain_sem)
    gain_copy.start()

    def fetch_weights():
        for j, w_hbm in enumerate(w_hbms):
            pltpu.make_async_copy(w_hbm, w_v.at[:, pl.ds(j * LANES, LANES)], w_sem).start()
        for j, vec_hbm in enumerate(vec_hbms):
            pltpu.make_async_copy(vec_hbm, vec_v.at[j], vec_sem).start()

    def st_copy(i):
        part = pl.ds(i * per, per)
        return pltpu.make_async_copy(st_hbm.at[part], st_v.at[part], st_sem.at[i])

    def ns_copy(i):
        part = pl.ds(i * per, per)
        return pltpu.make_async_copy(ns_v.at[part], ns_hbm.at[part], ns_sem)

    lane = lax.broadcasted_iota(jnp.int32, (seqs, LANES), 1)

    def per_head(values):
        first = jnp.sum(jnp.where(lane < HALF, values, 0.0), axis=1, keepdims=True)
        second = jnp.sum(jnp.where(lane < HALF, 0.0, values), axis=1, keepdims=True)
        return jnp.where(lane < HALF, first, second)

    wide = 2 * LANES
    block_r = lax.broadcasted_iota(jnp.int32, (wide, wide), 0) // HALF
    block_c = lax.broadcasted_iota(jnp.int32, (wide, wide), 1) // HALF
    diag = (
        lax.broadcasted_iota(jnp.int32, (HALF, LANES), 0)
        == lax.broadcasted_iota(jnp.int32, (HALF, LANES), 1) % HALF
    )[None]

    def old_state(part):
        return jnp.concatenate([st_v[part, 0], st_v[part, 1]], axis=-1)

    def row_of(j, part):
        return rows_v[j, part][:, None, :]

    def flat(values):
        return values.astype(BF16).reshape(PAIR * HALF, LANES)

    def head_sums(left, right):
        ones = (block_r == block_c).astype(BF16)
        both = dot(jnp.concatenate([flat(left), flat(right)], axis=1), ones)
        return (
            both[:, :LANES].reshape(PAIR, HALF, LANES),
            both[:, LANES:].reshape(PAIR, HALF, LANES),
        )

    def mixed_rows(fetch_rest):
        tok_copy.wait()
        for i in range(CHUNKS):
            st_copy(i).start()
        fetch_rest()
        values = tok_v[...].astype(F32)
        scale = lax.rsqrt(jnp.mean(values * values, axis=1, keepdims=True) + RMS_EPS)
        gain_copy.wait()
        normed = (values * scale * gain_v[...]).astype(BF16)
        pltpu.make_async_copy(w_v, w_v, w_sem).wait()
        pltpu.make_async_copy(vec_v, vec_v, vec_sem).wait()
        decay_base, rate_base, key_gain, group_gain = (vec_v[j] for j in range(4))
        projected = dot(normed, w_v[...]).astype(BF16).astype(F32)
        recept, key, value, decay_in, rate_in = (
            projected[:, j * LANES : (j + 1) * LANES] for j in range(5)
        )
        decay = jnp.exp(-(0.6065306597126334 * jax.nn.sigmoid(decay_in + decay_base)))
        rate = jax.nn.sigmoid(rate_in + rate_base)
        scaled = key * key_gain
        unit = scaled * lax.rsqrt(per_head(scaled * scaled) + UNIT_EPS)
        rows_v[0] = unit
        rows_v[1] = decay
        rows_v[2] = unit * rate
        rows_v[3] = key
        rows_v[4] = decay * recept
        rows_v[5] = value

        def look(i, carry):
            st_copy(i).wait()
            for p in range(per // PAIR):
                part = pl.ds(i * per + p * PAIR, PAIR)
                old = old_state(part)
                removed, seen = head_sums(old * row_of(0, part), old * row_of(4, part))
                read_v[0, part, :] = jnp.sum(jnp.where(diag, removed, 0.0), axis=1)
                read_v[1, part, :] = jnp.sum(jnp.where(diag, seen, 0.0), axis=1)
            return carry

        lax.fori_loop(0, CHUNKS, look, 0)
        taken = read_v[0] * per_head(unit * rate * recept)
        readout = read_v[1] - taken + value * per_head(key * recept)
        centred = readout - per_head(readout) * (1.0 / HALF)
        spread = per_head(centred * centred) * (1.0 / HALF)
        return (centred * lax.rsqrt(spread + GROUP_EPS) * group_gain).astype(BF16)

    def update():
        def chunk(i, carry):
            for p in range(per // PAIR):
                part = pl.ds(i * per + p * PAIR, PAIR)
                old = old_state(part)
                spread = jnp.where(diag, row_of(5, part), 0.0)
                removed, value = head_sums(old * row_of(0, part), spread)
                new = old * row_of(1, part) - removed * row_of(2, part) + value * row_of(3, part)
                ns_v[part] = new
            ns_copy(i).start()
            return carry

        lax.fori_loop(0, CHUNKS, chunk, 0)

    def finish():
        pltpu.make_async_copy(ns_v, ns_hbm, ns_sem).wait()

    return fetch_weights, mixed_rows, update, finish


def layer_kernel(
    tok_hbm,
    st_hbm,
    mix_gain_hbm,
    wr_hbm,
    wk_hbm,
    wv_hbm,
    wdec_hbm,
    wrate_hbm,
    decay_hbm,
    rate_hbm,
    key_hbm,
    group_hbm,
    routes_hbm,
    logits_hbm,
    gain_hbm,
    wo_hbm,
    wg_hbm,
    wu_hbm,
    wd_hbm,
    out_ref,
    ns_hbm,
    mtok_v,
    mgain_v,
    vec_v,
    w_v,
    st_v,
    ns_v,
    rows_v,
    read_v,
    tok_ref,
    routes_ref,
    logits_ref,
    gain_ref,
    wo_v,
    wg_v,
    wu_v,
    wd_v,
    pair_send,
    pair_recv,
    own_v,
    rs_send,
    rs_recv,
    resid_v,
    disp_send,
    x_recv,
    gate_v,
    up_v,
    y_send,
    y_recv,
    y_own,
    ret_send,
    ret_recv,
    moe_send,
    moe_recv,
    mtok_sem,
    mgain_sem,
    vec_sem,
    mw_sem,
    st_sem,
    ns_sem,
    in_sem,
    w_sem,
    send_sem,
    pair_sem,
    rs_sem,
    ag_sem,
    disp_sem,
    relay_sem,
    y_sem,
    ret_sem,
    moe_sem,
):
    depth = lax.axis_size("tp") // 2
    rows = tok_ref.shape[0]
    groups = SIDE * SIDE
    ep = lax.axis_index("ep")
    tp = lax.axis_index("tp")
    z, core = tp // 2, tp % 2
    y, x = ep // SIDE, ep % SIDE
    other = 1 - core

    def up_z(dz):
        return (z + dz) % depth

    def down_z(dz):
        return (z - dz + depth) % depth

    def along(dz):
        return (ep, up_z(dz) * 2 + core)

    def plane(o, sign):
        dy, dx = divmod(o, SIDE)
        to_y = (y + sign * dy + SIDE) % SIDE
        to_x = (x + sign * dx + SIDE) % SIDE
        return (to_y * SIDE + to_x, tp)

    partner = (ep, z * 2 + other)

    def send(src, dst, sender_sem, recv_sem, target):
        pltpu.make_async_remote_copy(
            src_ref=src,
            dst_ref=dst,
            send_sem=sender_sem,
            recv_sem=recv_sem,
            device_id=target,
            device_id_type=MESH,
        ).start()

    def take(ref, sem):
        pltpu.make_async_copy(ref, ref, sem).wait()

    def fetch(src, dst, sem):
        pltpu.make_async_copy(src, dst, sem).start()

    fetch_weights, mixed_rows, update, finish = mixer(
        (
            tok_hbm,
            st_hbm,
            mix_gain_hbm,
            (wr_hbm, wk_hbm, wv_hbm, wdec_hbm, wrate_hbm),
            (decay_hbm, rate_hbm, key_hbm, group_hbm),
            ns_hbm,
            mtok_v,
            mgain_v,
            vec_v,
            w_v,
            st_v,
            ns_v,
            rows_v,
            read_v,
            mtok_sem,
            mgain_sem,
            vec_sem,
            mw_sem,
            st_sem,
            ns_sem,
        )
    )
    barrier = pltpu.get_barrier_semaphore()
    peers = [partner] + [along(dz) for dz in range(1, depth)]
    peers += [plane(o, 1) for o in range(1, groups)]
    for peer in peers:
        pl.semaphore_signal(barrier, inc=1, device_id=peer, device_id_type=MESH)
    fetch_weights()

    def fetch_rest():
        for j in range(2 * depth):
            fetch(wo_hbm.at[:, pl.ds(j * LANES, LANES)], wo_v.at[j % 2, j // 2], in_sem.at[0])
        own_cols = pl.ds(pl.multiple_of(tp * LANES, LANES), LANES)
        fetch(routes_hbm, routes_ref, in_sem.at[1])
        fetch(logits_hbm, logits_ref, in_sem.at[2])
        fetch(tok_hbm.at[:, own_cols], tok_ref, in_sem.at[3])
        fetch(gain_hbm, gain_ref, in_sem.at[4])

    mixed = mixed_rows(fetch_rest)
    take(wo_v, in_sem.at[0])

    def wide(ref, side, blocks):
        return jnp.concatenate([ref[side, k] for k in blocks], axis=1)

    theirs = dot(mixed, wide(wo_v, other, range(depth))).astype(BF16)
    for k in range(depth):
        pair_send[k] = theirs[:, k * LANES : (k + 1) * LANES]
    pl.semaphore_wait(barrier, len(peers))
    send(pair_send, pair_recv, send_sem.at[0], pair_sem, partner)
    fetch(wg_hbm, wg_v, w_sem.at[0])
    fetch(wu_hbm, wu_v, w_sem.at[1])
    for j in range(2 * depth):
        fetch(wd_hbm.at[:, pl.ds(j * LANES, LANES)], wd_v.at[j % 2, j // 2], w_sem.at[2])
    mine = dot(mixed, wide(wo_v, core, range(depth)))
    for k in range(depth):
        own_v[k] = mine[:, k * LANES : (k + 1) * LANES]
    take(pair_recv, pair_sem)

    far = sorted(range(1, depth), key=lambda dz: -min(dz, depth - dz))
    for dz in far:
        k = up_z(dz)
        rs_send[dz] = (own_v[k] + pair_recv[k].astype(F32)).astype(BF16)
        send(rs_send.at[dz], rs_recv.at[dz], send_sem.at[1], rs_sem, along(dz))
    total = own_v[z] + pair_recv[z].astype(F32)

    for j, ref in enumerate((routes_ref, logits_ref, tok_ref, gain_ref)):
        take(ref, in_sem.at[1 + j])
    row16 = lax.broadcasted_iota(jnp.int32, (groups, rows), 0)
    expert = (((y + (row16 >> 2)) & 3) << 2) | ((x + (row16 & 3)) & 3)
    first = (routes_ref[0:1, :] == expert).astype(BF16)
    second = (routes_ref[1:2, :] == expert).astype(BF16)
    before = (
        lax.broadcasted_iota(jnp.int32, (rows, rows), 0)
        < lax.broadcasted_iota(jnp.int32, (rows, rows), 1)
    ).astype(BF16)
    rank = dot(first + second, before).astype(BF16)
    slots = groups * MAIN
    expand = (
        (lax.broadcasted_iota(jnp.int32, (slots, groups), 0) // MAIN)
        == lax.broadcasted_iota(jnp.int32, (slots, groups), 1)
    ).astype(BF16)
    first_x = dot(expand, first)
    second_x = dot(expand, second)
    rank_x = dot(expand, rank).astype(jnp.int32)
    slot = lax.broadcasted_iota(jnp.int32, (slots, rows), 0) % MAIN
    named = (first_x + second_x) > 0.5
    pick_main = jnp.where(named & (rank_x == slot), 1.0, 0.0)
    pick_low = jnp.where(named & (rank_x == slot + MAIN) & (slot < REST), 1.0, 0.0)
    pick_high = jnp.where(named & (rank_x == slot + REST) & (slot >= REST), 1.0, 0.0)
    exp0 = jnp.exp(logits_ref[0:1, :])
    exp1 = jnp.exp(logits_ref[1:2, :])
    weight = (first_x * exp0 + second_x * exp1) / (exp0 + exp1)

    def split(table):
        turned = (table * weight).T
        top = turned.astype(BF16)
        return jnp.concatenate([top, (turned - top.astype(F32)).astype(BF16)], axis=1)

    give_main = split(pick_main)
    give_rest = jnp.concatenate([split(pick_low), split(pick_high)], axis=0)
    pick_main, pick_low, pick_high = (t.astype(BF16) for t in (pick_main, pick_low, pick_high))

    update()
    take(rs_recv.at[pl.ds(1, depth - 1)], rs_sem)
    for dz in far:
        total = total + rs_recv[dz].astype(F32)
    own_resid = (tok_ref[...].astype(F32) + total).astype(BF16)
    resid_v[z] = own_resid

    ins = [(-j % depth, j + 1) for j in range(depth // 2)]
    pair_of = {dz: j for j, pair in enumerate(ins) for dz in pair}
    for dz in reversed(far):
        send(resid_v.at[z], resid_v.at[z], send_sem.at[2], ag_sem.at[pair_of[dz]], along(dz))
    two = 2 * LANES
    for j, (da, db) in enumerate(ins):
        if j:
            take(rs_recv.at[pl.ds(0, 2)], ag_sem.at[j])
        else:
            take(rs_recv.at[0], ag_sem.at[j])
        block_a, block_b = resid_v[down_z(da)], resid_v[down_z(db)]
        main = dot(pick_main, jnp.concatenate([block_a, block_b], axis=1)).astype(BF16)
        rest = (dot(pick_low, block_a) + dot(pick_high, block_b)).astype(BF16)
        disp_send[j, :, :, 0:two] = main.reshape(groups, MAIN, two)
        disp_send[j, :, :, two:] = rest.reshape(groups, MAIN, LANES)
        x_recv[core, j, 0] = disp_send[j, 0]
        for o in reversed(NEAR[1:]):
            src, dst = disp_send.at[j, o], x_recv.at[core, j, o]
            send(src, dst, send_sem.at[3], disp_sem.at[j], plane(o, 1))
    for j in range(len(ins)):
        take(x_recv.at[core, j, pl.ds(1, groups - 1)], disp_sem.at[j])
        block = x_recv.at[core, j]
        send(block, block, send_sem.at[4], relay_sem.at[j], partner)

    main_rows = groups * MAIN
    tile_row = lax.broadcasted_iota(jnp.int32, (groups // 2, MAIN, LANES), 1)
    upper = tile_row < REST
    squares = None
    for j, (da, db) in enumerate(ins):
        take(x_recv.at[other, j], relay_sem.at[j])
        if j == 0:
            take(wg_v, w_sem.at[0])
            take(wu_v, w_sem.at[1])
        mains, rests, gates, ups = [], [], [], []
        for p in range(2):
            got = x_recv[p, j].astype(F32)
            rest = got[:, :, two:].reshape(groups // 2, 2, MAIN, LANES)
            a, b = rest[:, 0], rest[:, 1]
            rest_a = jnp.where(upper, a, pltpu.roll(b, REST, 1)).reshape(-1, LANES)
            rest_b = jnp.where(upper, pltpu.roll(a, REST, 1), b).reshape(-1, LANES)
            for at, (dz, rest_d) in enumerate(((da, rest_a), (db, rest_b))):
                cols = pl.ds(pl.multiple_of((2 * down_z(dz) + p) * LANES, LANES), LANES)
                main = got[:, :, at * LANES : (at + 1) * LANES].reshape(main_rows, LANES)
                mains.append((main, gain_ref[:, cols]))
                rests.append((rest_d, gain_ref[:, cols]))
                gates.append(wg_v[:, cols])
                ups.append(wu_v[:, cols])
        parts = []
        for pieces in (mains, rests):
            squared = sum(jnp.sum(piece * piece, axis=1, keepdims=True) for piece, _ in pieces)
            scaled = jnp.concatenate([(piece * g).astype(BF16) for piece, g in pieces], axis=1)
            parts.append((squared, scaled))
        squared = jnp.concatenate([parts[0][0], parts[1][0]], axis=0)
        scaled = jnp.concatenate([parts[0][1], parts[1][1]], axis=0)
        gate = dot(scaled, jnp.concatenate(gates, axis=1), ((1,), (1,)))
        up = dot(scaled, jnp.concatenate(ups, axis=1), ((1,), (1,)))
        if j:
            squares = squares + squared
            gate = gate + gate_v[...]
            up = up + up_v[...]
        else:
            squares = squared
        if j < len(ins) - 1:
            gate_v[...] = gate
            up_v[...] = up
    scale = lax.rsqrt(squares * (1.0 / (2 * depth * LANES)) + RMS_EPS)
    gate = gate * scale
    hidden = (gate * jax.nn.sigmoid(gate) * (up * scale)).astype(BF16)

    take(wd_v, w_sem.at[2])
    outs = [(depth // 2 + j, depth // 2 - 1 - j) for j in range(depth // 2)]
    out_blocks = [up_z(dz) for pair in outs for dz in pair]
    theirs = dot(hidden, wide(wd_v, other, out_blocks)).astype(BF16)
    for j in range(len(outs)):
        y_send[j] = theirs[:, j * two : (j + 1) * two]
        send(y_send.at[j], y_recv.at[j], send_sem.at[5], y_sem.at[j], partner)
    mine = dot(hidden, wide(wd_v, core, out_blocks))
    for j in range(len(outs)):
        y_own[j] = mine[:, j * two : (j + 1) * two]
    for j in range(len(outs)):
        take(y_recv.at[j], y_sem.at[j])
        summed = y_own[j] + y_recv[j].astype(F32)
        ret_send[j, :, :, 0:two] = summed[:main_rows].astype(BF16).reshape(groups, MAIN, two)
        rest = summed[main_rows:].reshape(groups // 2, MAIN, two)
        rest_a, rest_b = rest[:, :, :LANES], rest[:, :, LANES:]
        even = jnp.where(upper, rest_a, pltpu.roll(rest_b, REST, 1)).astype(BF16)
        odd = jnp.where(upper, pltpu.roll(rest_a, REST, 1), rest_b).astype(BF16)
        for p in range(groups // 2):
            ret_send[j, 2 * p, :, two:] = even[p]
            ret_send[j, 2 * p + 1, :, two:] = odd[p]
        ret_recv[j, 0] = ret_send[j, 0]
        for o in reversed(NEAR[1:]):
            src, dst = ret_send.at[j, o], ret_recv.at[j, o]
            send(src, dst, send_sem.at[6], ret_sem.at[j], plane(o, -1))

    def give(tables, data):
        return dot(tables, jnp.concatenate([data, data], axis=0))

    for j, (da, db) in enumerate(outs):
        take(ret_recv.at[j, pl.ds(1, groups - 1)], ret_sem.at[j])
        back = ret_recv[j]
        main = give(give_main, back[:, :, :two].reshape(slots, two))
        rest = give(give_rest, back[:, :, two:].reshape(slots, LANES))
        for dz, moe in (
            (da, main[:, :LANES] + rest[:rows]),
            (db, main[:, LANES:] + rest[rows:]),
        ):
            if dz:
                moe_send[dz] = moe.astype(BF16)
                send(moe_send.at[dz], moe_recv.at[dz], send_sem.at[7], moe_sem, along(dz))
            else:
                total = own_resid.astype(F32) + moe
    take(moe_recv.at[pl.ds(1, depth - 1)], moe_sem)
    for dz in far:
        total = total + moe_recv[dz].astype(F32)
    out_ref[...] = total.astype(BF16)

    finish()
    seven = pl.ds(1, depth - 1)
    take(pair_send, send_sem.at[0])
    take(rs_send.at[seven], send_sem.at[1])
    take(rs_send.at[seven], send_sem.at[2])
    take(disp_send.at[:, pl.ds(1, groups - 1)], send_sem.at[3])
    take(x_recv.at[core], send_sem.at[4])
    take(y_send, send_sem.at[5])
    take(ret_send.at[:, pl.ds(1, groups - 1)], send_sem.at[6])
    take(moe_send.at[seven], send_sem.at[7])


def unpack_kernel(
    out_hbm, packed_hbm, copy_hbm, state_hbm, out_v, packed_v, state_v, out_sem, in_sem, st_sem
):
    per = packed_v.shape[0] // PIECES

    def piece(i):
        part = pl.ds(i * per, per)
        return pltpu.make_async_copy(packed_hbm.at[part], packed_v.at[part], in_sem.at[i])

    take_out = pltpu.make_async_copy(out_hbm, out_v, out_sem.at[0])
    take_out.start()
    for i in range(PIECES):
        piece(i).start()
    give_out = pltpu.make_async_copy(out_v, copy_hbm, out_sem.at[1])
    for i in range(PIECES):
        part = pl.ds(i * per, per)
        piece(i).wait()
        both = packed_v[part]
        state_v[part, 0] = both[..., :HALF]
        state_v[part, 1] = both[..., HALF:]
        pltpu.make_async_copy(state_v.at[part], state_hbm.at[part], st_sem).start()
        if i == 1:
            take_out.wait()
            give_out.start()
    give_out.wait()
    pltpu.make_async_copy(state_v, state_hbm, st_sem).wait()


def local(
    tokens,
    state,
    routes,
    route_logits,
    mix_gain,
    w_recept,
    w_key,
    w_value,
    w_decay,
    w_rate,
    decay_base,
    rate_base,
    key_gain,
    group_gain,
    w_output,
    ffn_gain,
    w_gate,
    w_up,
    w_down,
):
    seqs, width = tokens.shape
    hidden = w_gate.shape[2]
    vmem = pl.BlockSpec(memory_space=pltpu.VMEM)
    anywhere = pl.BlockSpec(memory_space=pl.ANY)
    dma = pltpu.SemaphoreType.DMA

    def row(vector):
        return vector.reshape(1, -1)

    depth = lax.axis_size("tp") // 2
    groups = SIDE * SIDE
    pairs = depth // 2
    message = (pairs, groups, MAIN, 3 * LANES)
    all_rows = groups * (MAIN + REST)
    block = (depth, seqs, LANES)
    packed = (seqs, state.shape[2], LANES)
    output, new_state = pl.pallas_call(
        layer_kernel,
        out_shape=(
            jax.ShapeDtypeStruct((seqs, LANES), BF16),
            jax.ShapeDtypeStruct(packed, F32),
        ),
        in_specs=[anywhere] * 19,
        out_specs=(vmem, anywhere),
        scratch_shapes=[
            pltpu.VMEM((seqs, width), BF16),
            pltpu.VMEM((1, width), F32),
            pltpu.VMEM((4, 1, LANES), F32),
            pltpu.VMEM((width, 5 * LANES), BF16),
            pltpu.VMEM(state.shape, F32),
            pltpu.VMEM(packed, F32),
            pltpu.VMEM((6, seqs, LANES), F32),
            pltpu.VMEM((2, seqs, LANES), F32),
            pltpu.VMEM((seqs, LANES), BF16),
            pltpu.VMEM(routes.shape[::-1], jnp.int32),
            pltpu.VMEM(routes.shape[::-1], F32),
            pltpu.VMEM((1, width), F32),
            pltpu.VMEM((2, depth, LANES, LANES), BF16),
            pltpu.VMEM((hidden, width), BF16),
            pltpu.VMEM((hidden, width), BF16),
            pltpu.VMEM((2, depth, hidden, LANES), BF16),
            pltpu.VMEM(block, BF16),
            pltpu.VMEM(block, BF16),
            pltpu.VMEM(block, F32),
            pltpu.VMEM(block, BF16),
            pltpu.VMEM(block, BF16),
            pltpu.VMEM(block, BF16),
            pltpu.VMEM(message, BF16),
            pltpu.VMEM((2,) + message, BF16),
            pltpu.VMEM((all_rows, hidden), F32),
            pltpu.VMEM((all_rows, hidden), F32),
            pltpu.VMEM((pairs, all_rows, 2 * LANES), BF16),
            pltpu.VMEM((pairs, all_rows, 2 * LANES), BF16),
            pltpu.VMEM((pairs, all_rows, 2 * LANES), F32),
            pltpu.VMEM(message, BF16),
            pltpu.VMEM(message, BF16),
            pltpu.VMEM(block, BF16),
            pltpu.VMEM(block, BF16),
            dma(()),
            dma(()),
            dma(()),
            dma(()),
            dma((CHUNKS,)),
            dma(()),
            dma((5,)),
            dma((3,)),
            dma((8,)),
            dma(()),
            dma(()),
            dma((pairs,)),
            dma((pairs,)),
            dma((pairs,)),
            dma((pairs,)),
            dma((pairs,)),
            dma(()),
        ],
        compiler_params=pltpu.CompilerParams(
            collective_id=0, has_side_effects=True, vmem_limit_bytes=GRANT
        ),
        name="layer",
    )(
        tokens,
        state,
        row(mix_gain),
        w_recept,
        w_key,
        w_value,
        w_decay,
        w_rate,
        row(decay_base),
        row(rate_base),
        row(key_gain),
        row(group_gain),
        routes.T,
        route_logits.T,
        row(ffn_gain),
        w_output,
        jnp.swapaxes(w_gate, 1, 2)[0],
        jnp.swapaxes(w_up, 1, 2)[0],
        w_down[0],
    )
    return pl.pallas_call(
        unpack_kernel,
        out_shape=(
            jax.ShapeDtypeStruct((seqs, LANES), BF16),
            jax.ShapeDtypeStruct(state.shape, F32),
        ),
        in_specs=[anywhere] * 2,
        out_specs=(anywhere, anywhere),
        scratch_shapes=[
            pltpu.VMEM((seqs, LANES), BF16),
            pltpu.VMEM(packed, F32),
            pltpu.VMEM(state.shape, F32),
            dma((2,)),
            dma((PIECES,)),
            dma(()),
        ],
        compiler_params=pltpu.CompilerParams(vmem_limit_bytes=GRANT),
        name="unpack",
    )(output, new_state)


def solution(mesh):
    return jax.shard_map(
        local,
        mesh=mesh,
        in_specs=(
            P("ep", None),
            P("ep", "tp", None, None),
            P("ep", None),
            P("ep", None),
            P(),
            P(None, "tp"),
            P(None, "tp"),
            P(None, "tp"),
            P(None, "tp"),
            P(None, "tp"),
            P("tp"),
            P("tp"),
            P("tp"),
            P("tp"),
            P("tp", None),
            P(),
            P("ep", None, "tp"),
            P("ep", None, "tp"),
            P("ep", "tp", None),
        ),
        out_specs=(P("ep", "tp"), P("ep", "tp", None, None)),
        check_vma=False,
    )
```
